32 devices in a mesh: sp: 8 (over z, x), tp: 4 (over y, core).
Axes of the slice: x: 2, y: 2, z: 4, core: 2. Of those that a mesh axis runs over, the one named last changes fastest.
Arguments:
- query_logits: bfloat16 [4096, 4096], P('sp', 'tp'), may hold values from -6 to 6
- forget_logits: bfloat16 [4096, 4096], P('sp', 'tp'), may hold values from -6 to 6
- value_inputs: bfloat16 [4096, 4096], P('sp', 'tp'), may hold values from -16 to 16
- output_gate_logits: bfloat16 [4096, 4096], P('sp', 'tp'), may hold values from -6 to 6
- forget_floor_gap: float32 [4096], replicated, may hold values from 2.4414063e-05 to 0.1
- surge_log_decay: float32 [32, 4096], P('tp', 'sp'), may hold values from -0.7 to 0
- head_norm_gain: float32 [128], replicated, may hold values from 0.1 to 1.9
- output_matrix: bfloat16 [4096, 4096], P('sp', 'tp'), may hold values from -1.25 to 1.25
- branch_norm_gain: float32 [4096], replicated, may hold values from 0.1 to 1.9
- residual: bfloat16 [4096, 4096], P('sp', 'tp'), may hold values from -6 to 6
Outputs:
- output: bfloat16 [4096, 4096], P('sp', 'tp')
The draws below stay inside these ranges and needn't reach their ends.
All inputs are finite; a program needn't handle non-finite values.
Results may differ from the reference program's by a relative error of at most 0.005.
Values may be sent and summed in bfloat16 or wider, within the bound.
A program may use at most 128 MiB of HBM per device.

```python
import math
import jax
import jax.numpy as jnp
from jax import lax

HEAD_DIM = 128
HEAD_TOTAL = 32
D = 4096
BLOCK_SPAN = 64
TOK_DEV = 512
TOKEN_TOTAL = 4096


surge_count = 3


def draw_forget_logits(key, part):
    leading_item, second = jax.random.split(key, 2)
    width = HEAD_TOTAL * HEAD_DIM
    offsets = jax.random.uniform(second, (TOKEN_TOTAL // TOK_DEV, 1, 1), jnp.float32, -1.5, 1.5)
    base = jnp.clip(jax.random.normal(leading_item, (TOKEN_TOTAL, width), jnp.float32), -4.0, 4.0)
    shifted = base.reshape(TOKEN_TOTAL // TOK_DEV, TOK_DEV, width) + offsets
    return shifted.reshape(TOKEN_TOTAL, width).astype(jnp.bfloat16)


def draw_forget_floor_gap(key, part):
    leading_item, second, third = jax.random.split(key, 3)
    share = 0.5
    quick = jax.random.uniform(leading_item, (HEAD_TOTAL, 1), jnp.float32) < share
    slow_gap = jax.random.uniform(second, (HEAD_TOTAL, HEAD_DIM), jnp.float32, 0.1, 0.6) / TOKEN_TOTAL
    quick_gap = jnp.exp(jax.random.uniform(third, (HEAD_TOTAL, HEAD_DIM), jnp.float32, math.log(0.03), math.log(0.1)))
    return jnp.where(quick, quick_gap, slow_gap).reshape(HEAD_TOTAL * HEAD_DIM)


def draw_surge_log_decay(key, part):
    leading_item, second = jax.random.split(key, 2)
    position_grid = jax.random.randint(leading_item, (HEAD_TOTAL, surge_count), 0, TOKEN_TOTAL)
    hits = jnp.any(jnp.arange(TOKEN_TOTAL)[None, :, None] == position_grid[:, None, :], axis=2)
    amounts = jnp.log(jax.random.uniform(second, (HEAD_TOTAL, TOKEN_TOTAL), jnp.float32, 0.5, 0.8))
    return jnp.where(hits, amounts, 0.0).astype(jnp.float32)


def draw_output_matrix(key, part):
    leading_item, second = jax.random.split(key, 2)
    width = HEAD_TOTAL * HEAD_DIM
    limit = 80.0 / math.sqrt(width)
    ramp = jnp.exp(math.log(3.0) * jnp.arange(D).astype(jnp.float32) / D)
    base = jnp.clip(jax.random.normal(leading_item, (width, D), jnp.float32), -4.0, 4.0)
    column_scale = ramp * jnp.exp(jax.random.uniform(second, (D,), jnp.float32, 0.0, math.log(4.0)))
    values = jnp.clip(base * column_scale / math.sqrt(width), -limit, limit)
    return values.astype(jnp.bfloat16)


def shard_levels(key, extent, cuts, least, top_value):
    def one(dim, parts):
        draws = jax.random.uniform(jax.random.fold_in(jax.random.fold_in(key, 6), dim), (parts,), jnp.float32, least / len(cuts), top_value / len(cuts))
        return jnp.repeat(jnp.exp(draws), extent[dim] // parts).reshape((-1,) + (1,) * (len(extent) - dim - 1))

    loudness = one(*cuts[0])
    for cut in cuts[1:]:
        loudness = loudness * one(*cut)
    return loudness


def noise(own_key, dims, deviation, reach, cuts=(), kind=jnp.bfloat16):
    values = jax.random.normal(own_key, dims, jnp.float32) * deviation
    if len(cuts) > 0:
        values = shard_levels(own_key, dims, cuts, -0.22, 0.18) * values
    return jnp.clip(values, min=-reach, max=reach).astype(kind)


def setup_inputs(seed: int = 0) -> dict:
    arg_keys = jax.random.split(jax.random.key(seed), 11)
    return {
        "query_logits": noise(arg_keys[0], (TOKEN_TOTAL, HEAD_TOTAL * HEAD_DIM), 1.0, 6.0, ((0, 8), (1, 4))),
        "forget_logits": draw_forget_logits(jax.random.fold_in(arg_keys[10], 71), 0),
        "value_inputs": noise(arg_keys[2], (TOKEN_TOTAL, HEAD_TOTAL * HEAD_DIM), 4.0, 16.0, ((0, 8), (1, 4))),
        "output_gate_logits": noise(arg_keys[3], (TOKEN_TOTAL, HEAD_TOTAL * HEAD_DIM), 1.0, 6.0, ((0, 8), (1, 4))),
        "forget_floor_gap": draw_forget_floor_gap(jax.random.fold_in(arg_keys[10], 71), 0),
        "surge_log_decay": draw_surge_log_decay(jax.random.fold_in(arg_keys[10], 71), 0),
        "head_norm_gain": jnp.clip(1.0 + 0.18 * jax.random.normal(arg_keys[6], (HEAD_DIM,), jnp.float32), 0.1, 1.9),
        "output_matrix": draw_output_matrix(jax.random.fold_in(arg_keys[10], 71), 0),
        "branch_norm_gain": jnp.clip(1.0 + 0.18 * jax.random.normal(arg_keys[8], (D,), jnp.float32), 0.1, 1.9),
        "residual": noise(arg_keys[9], (TOKEN_TOTAL, D), 1.0, 6.0, ((0, 8), (1, 4))),
    }


epsilon = 1e-06

def block_update(state, queries, keys_in, values_in, running):
    length = running.shape[1]
    middle = length // 2
    anchor = running[:, middle - 1:middle, :]
    ending = running[:, -1:, :]
    causal = jnp.tril(jnp.ones((length, length), dtype=bool))
    highest = lax.Precision.HIGHEST
    inter = jnp.einsum('htd,hde->hte', queries * jnp.exp(running), state, precision=highest)
    scores = jnp.einsum('htd,hsd->hts', queries * jnp.exp(running - anchor), keys_in * jnp.exp(anchor - running), precision=highest)
    intra = jnp.einsum('hts,hse->hte', jnp.where(causal[None], scores, 0.0), values_in, precision=highest)
    new_state = state * jnp.exp(ending[:, 0, :])[:, :, None] + jnp.einsum('hsd,hse->hde', keys_in * jnp.exp(ending - running), values_in, precision=highest)
    return (new_state, inter + intra)

def head_gates(query_logits, forget_logits, value_inputs, gap):
    row_count = query_logits.shape[0]
    head_count = query_logits.shape[1] // HEAD_DIM

    def shaped(array):
        return array.astype(jnp.float32).reshape(row_count, head_count, HEAD_DIM)
    queries = jax.nn.silu(shaped(query_logits)) * HEAD_DIM ** (-0.5)
    keys_in = gap.reshape(head_count, HEAD_DIM) * jax.nn.sigmoid(-shaped(forget_logits))
    values_in = shaped(value_inputs)
    decay_factors = jnp.log1p(-keys_in)
    return (queries, keys_in, values_in, decay_factors)

def gated_norm(heads_out, output_gate_logits, head_norm_gain):
    mean_sq = lax.optimization_barrier(jnp.mean(heads_out * heads_out, axis=-1, keepdims=True))
    gates = jax.nn.silu(output_gate_logits.astype(jnp.float32).reshape(heads_out.shape))
    normed = heads_out * lax.rsqrt(mean_sq + epsilon) * head_norm_gain * gates
    return normed.reshape(heads_out.shape[0], -1).astype(jnp.bfloat16)

def reference(query_logits, forget_logits, value_inputs, output_gate_logits, forget_floor_gap, surge_log_decay, head_norm_gain, output_matrix, branch_norm_gain, residual):
    number_of_blocks = TOKEN_TOTAL // BLOCK_SPAN

    def split_into_blocks(array):
        return array.reshape(number_of_blocks, BLOCK_SPAN, array.shape[1])
    surge_values = jnp.transpose(surge_log_decay).reshape(number_of_blocks, BLOCK_SPAN, HEAD_TOTAL)

    def step_forward(state, input_tuple):
        query_tile_block, forget_gate_block, value_rows_block, output_gate_block, surge_block, residual_block = input_tuple
        queries, keys_in, values_in, decay_factors = head_gates(query_tile_block, forget_gate_block, value_rows_block, forget_floor_gap)
        decay_factors = decay_factors + surge_block[:, :, None]
        running = jnp.cumsum(jnp.transpose(decay_factors, (1, 0, 2)), axis=1)
        new_state, heads_out = block_update(state, jnp.transpose(queries, (1, 0, 2)), jnp.transpose(keys_in, (1, 0, 2)), jnp.transpose(values_in, (1, 0, 2)), running)
        mixed_rows = gated_norm(jnp.transpose(heads_out, (1, 0, 2)), output_gate_block, head_norm_gain)
        projected = lax.optimization_barrier(jnp.dot(mixed_rows, output_matrix, preferred_element_type=jnp.float32).astype(jnp.bfloat16))
        branch = projected.astype(jnp.float32)
        scale = lax.rsqrt(lax.optimization_barrier(jnp.mean(branch * branch, axis=-1, keepdims=True)) + epsilon)
        result = (residual_block.astype(jnp.float32) + branch * scale * branch_norm_gain).astype(jnp.bfloat16)
        return (new_state, result)
    starting_state = jnp.zeros((HEAD_TOTAL, HEAD_DIM, HEAD_DIM), jnp.float32)
    unused_slot, output_list = lax.scan(step_forward, starting_state, (split_into_blocks(query_logits), split_into_blocks(forget_logits), split_into_blocks(value_inputs), split_into_blocks(output_gate_logits), surge_values, split_into_blocks(residual)))
    return output_list.reshape(TOKEN_TOTAL, D)
```

```python
import functools

import jax
import jax.numpy as jnp
from jax import lax
from jax.experimental import pallas as pl
from jax.experimental.pallas import tpu as pltpu
from jax.sharding import Mesh
from jax.sharding import PartitionSpec as P

HEAD_DIM = 128
SPAN = 128
EPSILON = 1e-06
NT = (((1,), (1,)), ((), ()))
TN = (((0,), (0,)), ((), ()))
NN = (((1,), (0,)), ((), ()))


def dot(a, b, dims=NN):
    return lax.dot_general(a, b, dims, preferred_element_type=jnp.float32)


def lower_triangle():
    rows = lax.broadcasted_iota(jnp.int32, (SPAN, SPAN), 0)
    columns = lax.broadcasted_iota(jnp.int32, (SPAN, SPAN), 1)
    return rows >= columns


def decays(forget_ref, gap, surge_ref, block, causal):
    rows = pl.ds(block * SPAN, SPAN)
    logits = forget_ref[rows, :].astype(jnp.float32)
    keys = gap / (1.0 + jnp.exp(logits))
    series = keys * (1.0 / 7.0) + (1.0 / 6.0)
    for order in (5, 4, 3, 2):
        series = series * keys + (1.0 / order)
    logs = -(series * keys + 1.0) * keys
    high = logs.astype(jnp.bfloat16)
    low = (logs - high.astype(jnp.float32)).astype(jnp.bfloat16)
    ones = causal.astype(jnp.bfloat16)
    surge = surge_ref[0, :, rows]
    surged = jnp.sum(jnp.where(causal, surge, 0.0), axis=1, keepdims=True)
    return keys, dot(ones, high) + dot(ones, low) + surged


def state_kernel(forget_ref, value_ref, gap_ref, surge_ref, state_ref, total_ref):
    causal = lower_triangle()
    gap = gap_ref[0]
    state = jnp.zeros((HEAD_DIM, HEAD_DIM), jnp.float32)
    total = jnp.zeros((1, HEAD_DIM), jnp.float32)
    for block in range(forget_ref.shape[0] // SPAN):
        keys, running = decays(forget_ref, gap, surge_ref, block, causal)
        ending = running[SPAN - 1 : SPAN, :]
        kept = (keys * jnp.exp(ending - running)).astype(jnp.bfloat16)
        values = value_ref[pl.ds(block * SPAN, SPAN), :]
        state = state * jnp.exp(ending) + dot(values, kept, TN)
        total = total + ending
    state_ref[0] = state.astype(jnp.bfloat16)
    total_ref[0] = jnp.broadcast_to(total, total_ref.shape[1:])


def output_kernel(
    query_ref, forget_ref, value_ref, gate_ref, gap_ref, surge_ref, gain_ref, carried_ref, mixed_ref
):
    causal = lower_triangle()
    gap = gap_ref[0]
    gain = gain_ref[...]
    state = carried_ref[0].astype(jnp.float32)
    middle = SPAN // 2
    count = forget_ref.shape[0] // SPAN
    for block in range(count):
        rows = pl.ds(block * SPAN, SPAN)
        keys, running = decays(forget_ref, gap, surge_ref, block, causal)
        anchor = running[middle - 1 : middle, :]
        ending = running[SPAN - 1 : SPAN, :]
        logits = query_ref[rows, :].astype(jnp.float32)
        queries = logits * (HEAD_DIM**-0.5) / (1.0 + jnp.exp(-logits))
        reach = queries * jnp.exp(running - anchor)
        back = keys * jnp.exp(anchor - running)
        values = value_ref[rows, :]
        scores = dot(reach.astype(jnp.bfloat16), back.astype(jnp.bfloat16), NT)
        scores = jnp.where(causal, scores, 0.0).astype(jnp.bfloat16)
        inter = dot(
            (reach * jnp.exp(anchor)).astype(jnp.bfloat16), state.astype(jnp.bfloat16), NT
        )
        out = inter + dot(scores, values)
        if block + 1 < count:
            kept = (back * jnp.exp(ending - anchor)).astype(jnp.bfloat16)
            state = state * jnp.exp(ending) + dot(values, kept, TN)
        mean_sq = jnp.mean(out * out, axis=1, keepdims=True)
        gates = gate_ref[rows, :].astype(jnp.float32)
        gates = gates / (1.0 + jnp.exp(-gates))
        mixed_ref[rows, :] = (out * lax.rsqrt(mean_sq + EPSILON) * gain * gates).astype(
            jnp.bfloat16
        )


def heads_call(kernel, arrays, specs, out_shape, out_specs, heads, flops, name):
    moved = sum(a.size * a.dtype.itemsize for a in arrays)
    return pl.pallas_call(
        kernel,
        grid=(heads,),
        in_specs=specs,
        out_specs=out_specs,
        out_shape=out_shape,
        name=name,
        compiler_params=pltpu.CompilerParams(vmem_limit_bytes=32 * 1024 * 1024),
        cost_estimate=pl.CostEstimate(flops=flops, bytes_accessed=moved, transcendentals=0),
    )(*arrays)


def product_kernel(order_ref, *refs):
    parts, weight_ref, out_ref = refs[:-2], refs[-2], refs[-1]
    depth = parts[0].shape[1]
    total = None
    for place, part in enumerate(parts):
        start = pl.multiple_of(order_ref[place] * depth, depth)
        term = dot(part[...], weight_ref[pl.ds(start, depth), :])
        total = term if total is None else total + term
    out_ref[...] = total.astype(out_ref.dtype)


def product(order, parts, weight, dtype):
    rows, columns = parts[0].shape[0], weight.shape[1]
    tile = 256
    depth = parts[0].shape[1]
    return pl.pallas_call(
        product_kernel,
        grid_spec=pltpu.PrefetchScalarGridSpec(
            num_scalar_prefetch=1,
            grid=(columns // tile,),
            in_specs=[pl.BlockSpec((rows, depth), lambda j, o: (0, 0)) for _ in parts]
            + [pl.BlockSpec((weight.shape[0], tile), lambda j, o: (0, j))],
            out_specs=pl.BlockSpec((rows, tile), lambda j, o: (0, j)),
        ),
        out_shape=jax.ShapeDtypeStruct((rows, columns), dtype),
        name="product",
        cost_estimate=pl.CostEstimate(
            flops=2 * rows * weight.shape[0] * columns,
            bytes_accessed=2 * (weight.size + rows * weight.shape[0]),
            transcendentals=0,
        ),
    )(order, *parts, weight)


def per_device(
    tp_size,
    sp_size,
    query_logits,
    forget_logits,
    value_inputs,
    output_gate_logits,
    forget_floor_gap,
    surge_log_decay,
    head_norm_gain,
    output_matrix,
    branch_norm_gain,
    residual,
):
    rows, width = query_logits.shape
    heads = width // HEAD_DIM
    column = lax.axis_index("tp")
    pair = lax.axis_index("lo")
    place = lax.axis_index("hi") * 2 + pair
    depth_each = output_matrix.shape[0]
    weight = lax.all_gather(output_matrix, "hi", axis=0, tiled=True)
    gap = lax.dynamic_slice_in_dim(
        forget_floor_gap.reshape(-1, 1, HEAD_DIM), column * heads, heads, axis=0
    )

    by_head = pl.BlockSpec((rows, HEAD_DIM), lambda h: (0, h))
    gap_spec = pl.BlockSpec((1, 1, HEAD_DIM), lambda h: (h, 0, 0))
    surge_spec = pl.BlockSpec((1, 1, rows), lambda h: (h, 0, 0))
    state_spec = pl.BlockSpec((1, HEAD_DIM, HEAD_DIM), lambda h: (h, 0, 0))
    total_spec = pl.BlockSpec((1, 8, HEAD_DIM), lambda h: (h, 0, 0))
    surge = surge_log_decay.reshape(heads, 1, rows)
    flops = heads * rows * HEAD_DIM * 400
    state, total = heads_call(
        state_kernel,
        (forget_logits, value_inputs, gap, surge),
        [by_head, by_head, gap_spec, surge_spec],
        (
            jax.ShapeDtypeStruct((heads, HEAD_DIM, HEAD_DIM), jnp.bfloat16),
            jax.ShapeDtypeStruct((heads, 8, HEAD_DIM), jnp.float32),
        ),
        (state_spec, total_spec),
        heads,
        flops,
        "states",
    )
    total = total[:, :1, :]

    axes = ("hi", "lo")

    def shifted(array, by):
        return lax.ppermute(array, axes, [(i, i + by) for i in range(sp_size - by)])

    state, total = shifted(state, 1), shifted(total, 1)
    by = 1
    while by < sp_size - 1:
        earlier, span = shifted(state, by), shifted(total, by)
        merged = earlier.astype(jnp.float32) * jnp.exp(total) + state.astype(jnp.float32)
        state = merged.astype(jnp.bfloat16)
        total = total + span
        by *= 2

    mixed = heads_call(
        output_kernel,
        (
            query_logits,
            forget_logits,
            value_inputs,
            output_gate_logits,
            gap,
            surge,
            head_norm_gain.reshape(1, HEAD_DIM),
            state,
        ),
        [by_head] * 4
        + [gap_spec, surge_spec, pl.BlockSpec((1, HEAD_DIM), lambda h: (0, 0)), state_spec],
        jax.ShapeDtypeStruct((rows, width), jnp.bfloat16),
        by_head,
        heads,
        2 * flops,
        "outputs",
    )

    split = mixed.reshape(rows, width // (2 * depth_each), 2, depth_each)

    def of_parity(parity):
        return lax.dynamic_index_in_dim(split, parity, axis=2, keepdims=False).reshape(
            rows, width // 2
        )

    swap = [(0, 1), (1, 0)]
    own = of_parity(pair)
    other = lax.ppermute(of_parity(1 - pair), "lo", swap)
    order, own_parts, other_parts = [column], [own], [other]
    stride = tp_size // 2
    while stride >= 1:
        pattern = [(i, i ^ stride) for i in range(tp_size)]
        other_parts = other_parts + [lax.ppermute(p, "tp", pattern) for p in other_parts]
        own_parts = own_parts + [lax.ppermute(p, "tp", pattern) for p in own_parts]
        order = order + [o ^ stride for o in order]
        stride //= 2
    order = jnp.stack(order).astype(jnp.int32)
    away = product(order, other_parts, weight, jnp.bfloat16)
    arrived = lax.ppermute(away, "lo", swap)
    here = product(order, own_parts, weight, jnp.float32)
    projected = (here + arrived.astype(jnp.float32)).astype(jnp.bfloat16)
    branch = lax.optimization_barrier(projected).astype(jnp.float32)
    squares = lax.psum(jnp.sum(branch * branch, axis=1), "tp")
    columns = branch.shape[1]
    scale = lax.rsqrt(squares / (columns * tp_size) + EPSILON)
    gain_part = lax.dynamic_slice_in_dim(branch_norm_gain, column * columns, columns)
    return (residual.astype(jnp.float32) + branch * scale[:, None] * gain_part).astype(jnp.bfloat16)


def solution(mesh):
    sp_size, tp_size = mesh.shape["sp"], mesh.shape["tp"]
    paired = Mesh(mesh.devices.reshape(sp_size // 2, 2, tp_size), ("hi", "lo", "tp"))
    sp = ("hi", "lo")
    placed = (
        P(sp, "tp"),
        P(sp, "tp"),
        P(sp, "tp"),
        P(sp, "tp"),
        P(),
        P("tp", sp),
        P(),
        P(sp, "tp"),
        P(),
        P(sp, "tp"),
    )
    return jax.shard_map(
        functools.partial(per_device, tp_size, sp_size),
        mesh=paired,
        in_specs=placed,
        out_specs=P(sp, "tp"),
        check_vma=False,
    )
```

```python
import functools

import jax
import jax.numpy as jnp
from jax import lax
from jax.experimental import pallas as pl
from jax.experimental.pallas import tpu as pltpu
from jax.sharding import Mesh
from jax.sharding import PartitionSpec as P

HEAD_DIM = 128
SPAN = 128
EPSILON = 1e-06
NT = (((1,), (1,)), ((), ()))
TN = (((0,), (0,)), ((), ()))
NN = (((1,), (0,)), ((), ()))


def dot(a, b, dims=NN):
    return lax.dot_general(a, b, dims, preferred_element_type=jnp.float32)


def lower_triangle():
    rows = lax.broadcasted_iota(jnp.int32, (SPAN, SPAN), 0)
    columns = lax.broadcasted_iota(jnp.int32, (SPAN, SPAN), 1)
    return rows >= columns


def decays(logits, gap, surge, causal):
    keys = gap / (1.0 + jnp.exp(logits.astype(jnp.float32)))
    series = keys * (1.0 / 7.0) + (1.0 / 6.0)
    for order in (5, 4, 3, 2):
        series = series * keys + (1.0 / order)
    logs = -(series * keys + 1.0) * keys
    high = logs.astype(jnp.bfloat16)
    low = (logs - high.astype(jnp.float32)).astype(jnp.bfloat16)
    ones = causal.astype(jnp.bfloat16)
    surged = jnp.sum(jnp.where(causal, surge, 0.0), axis=1, keepdims=True)
    return keys, dot(ones, high) + dot(ones, low) + surged


def head_state(lanes, head, rows, forget_ref, value_ref, gap_ref, surge_ref):
    causal = lower_triangle()
    gap = gap_ref[head]
    state = jnp.zeros((HEAD_DIM, HEAD_DIM), jnp.float32)
    total = jnp.zeros((1, HEAD_DIM), jnp.float32)
    for start in range(0, rows, SPAN):
        span = pl.ds(start, SPAN)
        keys, running = decays(forget_ref[span, lanes], gap, surge_ref[head, :, span], causal)
        ending = running[SPAN - 1 : SPAN, :]
        kept = (keys * jnp.exp(ending - running)).astype(jnp.bfloat16)
        state = state * jnp.exp(ending) + dot(value_ref[span, lanes], kept, TN)
        total = total + ending
    return state, total


def head_output(
    lanes, head, rows, query_ref, forget_ref, value_ref, gate_ref, gap_ref, surge_ref, gain, state, put
):
    causal = lower_triangle()
    gap = gap_ref[head]
    middle = SPAN // 2
    for start in range(0, rows, SPAN):
        span = pl.ds(start, SPAN)
        keys, running = decays(forget_ref[span, lanes], gap, surge_ref[head, :, span], causal)
        anchor = running[middle - 1 : middle, :]
        ending = running[SPAN - 1 : SPAN, :]
        logits = query_ref[span, lanes].astype(jnp.float32)
        queries = logits * (HEAD_DIM**-0.5) / (1.0 + jnp.exp(-logits))
        reach = queries * jnp.exp(running - anchor)
        back = keys * jnp.exp(anchor - running)
        values = value_ref[span, lanes]
        scores = dot(reach.astype(jnp.bfloat16), back.astype(jnp.bfloat16), NT)
        scores = jnp.where(causal, scores, 0.0).astype(jnp.bfloat16)
        inter = dot(
            (reach * jnp.exp(anchor)).astype(jnp.bfloat16), state.astype(jnp.bfloat16), NT
        )
        out = inter + dot(scores, values)
        if start + SPAN < rows:
            kept = (back * jnp.exp(ending - anchor)).astype(jnp.bfloat16)
            state = state * jnp.exp(ending) + dot(values, kept, TN)
        mean_sq = jnp.mean(out * out, axis=1, keepdims=True)
        gates = gate_ref[span, lanes].astype(jnp.float32)
        gates = gates / (1.0 + jnp.exp(-gates))
        put(span, (out * lax.rsqrt(mean_sq + EPSILON) * gain * gates).astype(jnp.bfloat16))


MESH_ID = pl.DeviceIdType.MESH


def front_kernel(
    sizes,
    query_ref,
    forget_ref,
    value_ref,
    gate_ref,
    gap_ref,
    surge_ref,
    gain_ref,
    parts_ref,
    state_out,
    total_out,
    state_in,
    total_in,
    carried,
    span_total,
    away,
    state_sems,
    total_sems,
    swap_sems,
    tp_sems,
):
    hi_size, inner_size, tp_size, block = sizes
    sp_size = 2 * hi_size * inner_size
    rows, width = query_ref.shape
    heads = width // HEAD_DIM
    half = heads // 2
    per = block // HEAD_DIM
    lo, inner, tp = (lax.axis_index(a) for a in ("lo", "inner", "tp"))
    place = (lax.axis_index("hi") * 2 + lo) * inner_size + inner

    def at(position):
        return {
            "hi": position // (2 * inner_size),
            "lo": (position // inner_size) % 2,
            "inner": position % inner_size,
        }

    shifts = [1]
    by = 1
    while by < sp_size - 1:
        shifts.append(by)
        by *= 2
    strides = []
    stride = tp_size // 2
    while stride >= 1:
        strides.append(stride)
        stride //= 2

    def flipped(stride):
        return tp + stride - 2 * stride * ((tp // stride) % 2)

    barrier = pltpu.get_barrier_semaphore()
    reaches = sorted(set(shifts + [inner_size]))
    peers = len(strides)
    for by in reaches:
        for there in (place + by, place - by):
            inside = (there >= 0) & (there < sp_size)

            @pl.when(inside)
            def _():
                pl.semaphore_signal(barrier, inc=1, device_id=at(there), device_id_type=MESH_ID)

            peers = peers + jnp.where(inside, 1, 0)
    for stride in strides:
        pl.semaphore_signal(
            barrier, inc=1, device_id={"tp": flipped(stride)}, device_id_type=MESH_ID
        )
    pl.semaphore_wait(barrier, peers)

    def lanes_of(head):
        return pl.ds(pl.multiple_of(head * HEAD_DIM, HEAD_DIM), HEAD_DIM)

    def state_body(head, carry):
        state, total = head_state(
            lanes_of(head), head, rows, forget_ref, value_ref, gap_ref, surge_ref
        )
        state_out[0, head] = state.astype(jnp.bfloat16)
        total_out[0, head] = jnp.broadcast_to(total, (8, HEAD_DIM))
        return carry

    lax.fori_loop(0, heads, state_body, 0)

    for turn, by in enumerate(shifts):
        copies = [
            pltpu.make_async_remote_copy(
                src_ref=source.at[turn],
                dst_ref=target.at[turn],
                send_sem=sems.at[0, turn],
                recv_sem=sems.at[1, turn],
                device_id=at(place + by),
                device_id_type=MESH_ID,
            )
            for source, target, sems in (
                (state_out, state_in, state_sems),
                (total_out, total_in, total_sems),
            )
        ]

        @pl.when(place + by < sp_size)
        def _():
            for copy in copies:
                copy.start()

        if turn == 0:

            @pl.when(place == 0)
            def _():
                carried[...] = jnp.zeros_like(carried)
                span_total[...] = jnp.zeros_like(span_total)

        @pl.when(place - by >= 0)
        def _():
            for copy in copies:
                copy.wait_recv()

            def merge(head, carry):
                arrived = state_in[turn, head].astype(jnp.float32)
                passed = total_in[turn, head]
                if turn == 0:
                    carried[head] = arrived
                    span_total[head] = passed
                else:
                    carried[head] = arrived * jnp.exp(span_total[head, 0:1, :]) + carried[head]
                    span_total[head] = span_total[head] + passed
                return carry

            lax.fori_loop(0, heads, merge, 0)

        if turn + 1 < len(shifts):
            state_out[turn + 1] = carried[...].astype(jnp.bfloat16)
            total_out[turn + 1] = span_total[...]

    gain = gain_ref[...]

    def compute(head, put):
        head_output(
            lanes_of(head),
            head,
            rows,
            query_ref,
            forget_ref,
            value_ref,
            gate_ref,
            gap_ref,
            surge_ref,
            gain,
            carried[head],
            put,
        )

    def head_of(chunk, parity):
        return (chunk // per * 2 + parity) * per + chunk % per

    def columns(chunk):
        return pl.ds(pl.multiple_of(chunk * HEAD_DIM, HEAD_DIM), HEAD_DIM)

    def swap_copy(chunk):
        return pltpu.make_async_remote_copy(
            src_ref=away.at[:, columns(chunk)],
            dst_ref=parts_ref.at[1, tp, :, columns(chunk)],
            send_sem=swap_sems.at[0, chunk],
            recv_sem=swap_sems.at[1, chunk],
            device_id={"lo": 1 - lo},
            device_id_type=MESH_ID,
        )

    def tp_copy(stage, which, mine, chunk):
        slot = tp
        for bit, stride in enumerate(strides[:stage]):
            if (mine >> bit) & 1:
                slot = slot + stride - 2 * stride * ((tp // stride) % 2)
        return pltpu.make_async_remote_copy(
            src_ref=parts_ref.at[which, slot, :, columns(chunk)],
            dst_ref=parts_ref.at[which, slot, :, columns(chunk)],
            send_sem=tp_sems.at[0, stage, which, mine, chunk],
            recv_sem=tp_sems.at[1, stage, which, mine, chunk],
            device_id={"tp": flipped(strides[stage])},
            device_id_type=MESH_ID,
        )

    def away_body(chunk, carry):
        def put(span, value):
            away[span, columns(chunk)] = value

        compute(head_of(chunk, 1 - lo), put)
        swap_copy(chunk).start()
        return carry

    lax.fori_loop(0, half, away_body, 0)

    def own_body(chunk, carry):
        def put(span, value):
            parts_ref[0, tp, span, columns(chunk)] = value

        compute(head_of(chunk, lo), put)
        for stage in range(len(strides)):
            tp_copy(stage, 0, 0, chunk).start()
        swap_copy(chunk).wait_recv()
        for stage in range(len(strides)):
            tp_copy(stage, 1, 0, chunk).start()
        return carry

    lax.fori_loop(0, half, own_body, 0)

    for stage in range(len(strides)):

        def pass_body(chunk, carry):
            for which in (0, 1):
                for mine in range(1 << stage):
                    tp_copy(stage, which, mine, chunk).wait_recv()
                    for later in range(stage + 1, len(strides)):
                        tp_copy(later, which, mine | (1 << stage), chunk).start()
            return carry

        lax.fori_loop(0, half, pass_body, 0)

    for turn, by in enumerate(shifts):

        @pl.when(place + by < sp_size)
        def _():
            for source, target, sems in (
                (state_out, state_in, state_sems),
                (total_out, total_in, total_sems),
            ):
                pltpu.make_async_remote_copy(
                    src_ref=source.at[turn],
                    dst_ref=target.at[turn],
                    send_sem=sems.at[0, turn],
                    recv_sem=sems.at[1, turn],
                    device_id=at(place + by),
                    device_id_type=MESH_ID,
                ).wait_send()

    def sent_body(chunk, carry):
        swap_copy(chunk).wait_send()
        for stage in range(len(strides)):
            for which in (0, 1):
                for mine in range(1 << stage):
                    tp_copy(stage, which, mine, chunk).wait_send()
        return carry

    lax.fori_loop(0, half, sent_body, 0)


def front(sizes, query_logits, forget_logits, value_inputs, gate_logits, gap, surge, gain):
    hi_size, inner_size, tp_size, block = sizes
    rows, width = query_logits.shape
    heads = width // HEAD_DIM
    turns = 1 + (2 * hi_size * inner_size - 2).bit_length()
    stages = tp_size.bit_length() - 1
    vmem = pl.BlockSpec(memory_space=pltpu.VMEM)
    state = (heads, HEAD_DIM, HEAD_DIM)
    return pl.pallas_call(
        functools.partial(front_kernel, sizes),
        in_specs=[vmem] * 7,
        out_specs=vmem,
        out_shape=jax.ShapeDtypeStruct((2, tp_size, rows, width // 2), jnp.bfloat16),
        scratch_shapes=[
            pltpu.VMEM((turns,) + state, jnp.bfloat16),
            pltpu.VMEM((turns, heads, 8, HEAD_DIM), jnp.float32),
            pltpu.VMEM((turns,) + state, jnp.bfloat16),
            pltpu.VMEM((turns, heads, 8, HEAD_DIM), jnp.float32),
            pltpu.VMEM(state, jnp.float32),
            pltpu.VMEM((heads, 8, HEAD_DIM), jnp.float32),
            pltpu.VMEM((rows, width // 2), jnp.bfloat16),
            pltpu.SemaphoreType.DMA((2, turns)),
            pltpu.SemaphoreType.DMA((2, turns)),
            pltpu.SemaphoreType.DMA((2, heads // 2)),
            pltpu.SemaphoreType.DMA((2, stages, 2, tp_size // 2, heads // 2)),
        ],
        name="front",
        compiler_params=pltpu.CompilerParams(
            collective_id=0, has_side_effects=True, vmem_limit_bytes=48 * 1024 * 1024
        ),
        cost_estimate=pl.CostEstimate(
            flops=rows * width * 2000, bytes_accessed=8 * rows * width, transcendentals=0
        ),
    )(query_logits, forget_logits, value_inputs, gate_logits, gap, surge, gain)


def product_kernel(parts_ref, weight_ref, out_ref):
    depth = parts_ref.shape[-1]
    total = None
    for place in range(parts_ref.shape[1]):
        term = dot(parts_ref[0, place], weight_ref[pl.ds(place * depth, depth), :])
        total = term if total is None else total + term
    out_ref[...] = total.astype(out_ref.dtype)


def product(which, parts, weight, dtype):
    rows, columns = parts.shape[2], weight.shape[1]
    tile = 256
    return pl.pallas_call(
        product_kernel,
        grid=(columns // tile,),
        in_specs=[
            pl.BlockSpec((1,) + parts.shape[1:], lambda j: (which, 0, 0, 0)),
            pl.BlockSpec((weight.shape[0], tile), lambda j: (0, j)),
        ],
        out_specs=pl.BlockSpec((rows, tile), lambda j: (0, j)),
        out_shape=jax.ShapeDtypeStruct((rows, columns), dtype),
        name="product",
        cost_estimate=pl.CostEstimate(
            flops=2 * rows * weight.shape[0] * columns,
            bytes_accessed=2 * (weight.size + rows * weight.shape[0]),
            transcendentals=0,
        ),
    )(parts, weight)


def per_device(
    hi_size,
    inner_size,
    tp_size,
    query_logits,
    forget_logits,
    value_inputs,
    output_gate_logits,
    forget_floor_gap,
    surge_log_decay,
    head_norm_gain,
    output_matrix,
    branch_norm_gain,
    residual,
):
    rows, width = query_logits.shape
    heads = width // HEAD_DIM
    column = lax.axis_index("tp")
    weight = lax.all_gather(output_matrix, ("hi", "inner"), axis=0, tiled=True)
    gap = lax.dynamic_slice_in_dim(
        forget_floor_gap.reshape(-1, 1, HEAD_DIM), column * heads, heads, axis=0
    )
    parts = front(
        (hi_size, inner_size, tp_size, inner_size * output_matrix.shape[0]),
        query_logits,
        forget_logits,
        value_inputs,
        output_gate_logits,
        gap,
        surge_log_decay.reshape(heads, 1, rows),
        head_norm_gain.reshape(1, HEAD_DIM),
    )
    away = product(1, parts, weight, jnp.bfloat16)
    arrived = lax.ppermute(away, "lo", [(0, 1), (1, 0)])
    here = product(0, parts, weight, jnp.float32)
    projected = (here + arrived.astype(jnp.float32)).astype(jnp.bfloat16)
    branch = lax.optimization_barrier(projected).astype(jnp.float32)
    squares = lax.psum(jnp.sum(branch * branch, axis=1), "tp")
    columns = branch.shape[1]
    scale = lax.rsqrt(squares / (columns * tp_size) + EPSILON)
    gain_part = lax.dynamic_slice_in_dim(branch_norm_gain, column * columns, columns)
    return (residual.astype(jnp.float32) + branch * scale[:, None] * gain_part).astype(jnp.bfloat16)


def solution(mesh):
    sp_size, tp_size = mesh.shape["sp"], mesh.shape["tp"]
    sp = ("hi", "lo", "inner")
    placed = (
        P(sp, "tp"),
        P(sp, "tp"),
        P(sp, "tp"),
        P(sp, "tp"),
        P(),
        P("tp", sp),
        P(),
        P(sp, "tp"),
        P(),
        P(sp, "tp"),
    )

    def whole(*arrays):
        inner = max(1, HEAD_DIM * sp_size // arrays[7].shape[0])
        hi = sp_size // (2 * inner)
        devices = mesh.devices.reshape(hi, 2, inner, tp_size)
        paired = Mesh(devices, ("hi", "lo", "inner", "tp"))
        return jax.shard_map(
            functools.partial(per_device, hi, inner, tp_size),
            mesh=paired,
            in_specs=placed,
            out_specs=P(sp, "tp"),
            check_vma=False,
        )(*arrays)

    return whole
```

```python
import functools

import jax
import jax.numpy as jnp
from jax import lax
from jax.experimental import pallas as pl
from jax.experimental.pallas import tpu as pltpu
from jax.sharding import Mesh
from jax.sharding import PartitionSpec as P

HEAD_DIM = 128
SPAN = 128
EPSILON = 1e-06
NT = (((1,), (1,)), ((), ()))
TN = (((0,), (0,)), ((), ()))
NN = (((1,), (0,)), ((), ()))


def dot(a, b, dims=NN):
    return lax.dot_general(a, b, dims, preferred_element_type=jnp.float32)


def lower_triangle():
    rows = lax.broadcasted_iota(jnp.int32, (SPAN, SPAN), 0)
    columns = lax.broadcasted_iota(jnp.int32, (SPAN, SPAN), 1)
    return rows >= columns


def decays(logits, gap, surge, causal):
    keys = gap / (1.0 + jnp.exp(logits.astype(jnp.float32)))
    series = keys * (1.0 / 7.0) + (1.0 / 6.0)
    for order in (5, 4, 3, 2):
        series = series * keys + (1.0 / order)
    logs = -(series * keys + 1.0) * keys
    high = logs.astype(jnp.bfloat16)
    low = (logs - high.astype(jnp.float32)).astype(jnp.bfloat16)
    ones = causal.astype(jnp.bfloat16)
    surged = jnp.sum(jnp.where(causal, surge, 0.0), axis=1, keepdims=True)
    return keys, dot(ones, high) + dot(ones, low) + surged


def head_state(lanes, head, rows, forget_ref, value_ref, gap_ref, surge_ref):
    causal = lower_triangle()
    gap = gap_ref[head]
    state = jnp.zeros((HEAD_DIM, HEAD_DIM), jnp.float32)
    total = jnp.zeros((1, HEAD_DIM), jnp.float32)
    for start in range(0, rows, SPAN):
        span = pl.ds(start, SPAN)
        keys, running = decays(forget_ref[span, lanes], gap, surge_ref[head, :, span], causal)
        ending = running[SPAN - 1 : SPAN, :]
        kept = (keys * jnp.exp(ending - running)).astype(jnp.bfloat16)
        state = state * jnp.exp(ending) + dot(value_ref[span, lanes], kept, TN)
        total = total + ending
    return state, total


def head_output(
    lanes, head, rows, query_ref, forget_ref, value_ref, gate_ref, gap_ref, surge_ref, gain, state, put
):
    causal = lower_triangle()
    gap = gap_ref[head]
    middle = SPAN // 2
    for start in range(0, rows, SPAN):
        span = pl.ds(start, SPAN)
        keys, running = decays(forget_ref[span, lanes], gap, surge_ref[head, :, span], causal)
        anchor = running[middle - 1 : middle, :]
        ending = running[SPAN - 1 : SPAN, :]
        logits = query_ref[span, lanes].astype(jnp.float32)
        queries = logits * (HEAD_DIM**-0.5) / (1.0 + jnp.exp(-logits))
        reach = queries * jnp.exp(running - anchor)
        back = keys * jnp.exp(anchor - running)
        values = value_ref[span, lanes]
        scores = dot(reach.astype(jnp.bfloat16), back.astype(jnp.bfloat16), NT)
        scores = jnp.where(causal, scores, 0.0).astype(jnp.bfloat16)
        inter = dot(
            (reach * jnp.exp(anchor)).astype(jnp.bfloat16), state.astype(jnp.bfloat16), NT
        )
        out = inter + dot(scores, values)
        if start + SPAN < rows:
            kept = (back * jnp.exp(ending - anchor)).astype(jnp.bfloat16)
            state = state * jnp.exp(ending) + dot(values, kept, TN)
        mean_sq = jnp.mean(out * out, axis=1, keepdims=True)
        gates = gate_ref[span, lanes].astype(jnp.float32)
        gates = gates / (1.0 + jnp.exp(-gates))
        put(span, (out * lax.rsqrt(mean_sq + EPSILON) * gain * gates).astype(jnp.bfloat16))


MESH_ID = pl.DeviceIdType.MESH


def front_kernel(
    sizes,
    query_in,
    forget_in,
    value_in,
    gate_in,
    gap_ref,
    surge_ref,
    gain_ref,
    weight_ref,
    projected_ref,
    parts_ref,
    whole_weight,
    state_out,
    total_out,
    state_in,
    total_in,
    carried,
    span_total,
    away,
    query_ref,
    forget_ref,
    value_ref,
    gate_ref,
    partial_out,
    partial_in,
    here,
    state_sems,
    total_sems,
    swap_sems,
    tp_sems,
    load_sems,
    weight_sems,
    partial_sems,
):
    hi_size, inner_size, tp_size, block = sizes
    sp_size = 2 * hi_size * inner_size
    rows, width = query_in.shape
    heads = width // HEAD_DIM
    half = heads // 2
    per = block // HEAD_DIM
    lo, inner, tp = (lax.axis_index(a) for a in ("lo", "inner", "tp"))
    place = (lax.axis_index("hi") * 2 + lo) * inner_size + inner

    def at(position):
        return {
            "hi": position // (2 * inner_size),
            "lo": (position // inner_size) % 2,
            "inner": position % inner_size,
        }

    shifts = [1]
    by = 1
    while by < sp_size - 1:
        shifts.append(by)
        by *= 2
    strides = []
    stride = tp_size // 2
    while stride >= 1:
        strides.append(stride)
        stride //= 2

    def flipped(stride):
        return tp + stride - 2 * stride * ((tp // stride) % 2)

    line = hi_size * inner_size
    spot = lax.axis_index("hi") * inner_size + inner
    depth = weight_ref.shape[0]
    pieces, _, tile = partial_out.shape

    def slot(number):
        return pl.ds(pl.multiple_of(number * depth, depth), depth)

    loads = [
        pltpu.make_async_copy(source, target, load_sems.at[number])
        for number, (source, target) in enumerate(
            (
                (weight_ref, whole_weight.at[slot(spot)]),
                (forget_in, forget_ref),
                (value_in, value_ref),
                (query_in, query_ref),
                (gate_in, gate_ref),
            )
        )
    ]
    for load in loads:
        load.start()

    def on_line(position):
        return {"hi": position // inner_size, "inner": position % inner_size}

    def weight_copy(way, hop, piece):
        step = 1 if way == 0 else -1
        block = whole_weight.at[slot(spot - step * (hop - 1)), pl.ds(piece * tile, tile)]
        return pltpu.make_async_remote_copy(
            src_ref=block,
            dst_ref=block,
            send_sem=weight_sems.at[0, way, hop - 1, piece],
            recv_sem=weight_sems.at[1, way, hop - 1, piece],
            device_id=on_line(spot + step),
            device_id_type=MESH_ID,
        )

    def sends(way, hop):
        step = 1 if way == 0 else -1
        origin = spot - step * (hop - 1)
        target = spot + step
        return (origin >= 0) & (origin < line) & (target >= 0) & (target < line)

    def receives(way, hop):
        origin = spot - (1 if way == 0 else -1) * hop
        return (origin >= 0) & (origin < line)

    def send_weight(way, hop, piece):
        @pl.when(sends(way, hop))
        def _():
            weight_copy(way, hop, piece).start()

    def take_weight(hop, piece):
        for way in (0, 1):

            @pl.when(receives(way, hop))
            def _():
                weight_copy(way, hop, piece).wait_recv()

            if hop + 1 < line:
                send_weight(way, hop + 1, piece)

    def take_hop(hop):
        for piece in range(pieces):
            take_weight(hop, piece)

    barrier = pltpu.get_barrier_semaphore()
    reaches = sorted(set(shifts + [inner_size]))
    neighbours = [spot + 1, spot - 1]
    peers = len(strides)
    for by in reaches:
        for there in (place + by, place - by):
            inside = (there >= 0) & (there < sp_size)

            @pl.when(inside)
            def _():
                pl.semaphore_signal(barrier, inc=1, device_id=at(there), device_id_type=MESH_ID)

            peers = peers + jnp.where(inside, 1, 0)
    for there in neighbours:
        inside = (there >= 0) & (there < line)

        @pl.when(inside)
        def _():
            pl.semaphore_signal(barrier, inc=1, device_id=on_line(there), device_id_type=MESH_ID)

        peers = peers + jnp.where(inside, 1, 0)
    for stride in strides:
        pl.semaphore_signal(
            barrier, inc=1, device_id={"tp": flipped(stride)}, device_id_type=MESH_ID
        )
    pl.semaphore_wait(barrier, peers)
    loads[0].wait()
    late = pieces // 2
    for piece in range(pieces):
        send_weight(1, 1, piece)
        if piece < late:
            send_weight(0, 1, piece)
    loads[1].wait()
    loads[2].wait()

    def lanes_of(head):
        return pl.ds(pl.multiple_of(head * HEAD_DIM, HEAD_DIM), HEAD_DIM)

    def state_body(head, carry):
        state, total = head_state(
            lanes_of(head), head, rows, forget_ref, value_ref, gap_ref, surge_ref
        )
        state_out[0, head] = state.astype(jnp.bfloat16)
        total_out[0, head] = jnp.broadcast_to(total, (8, HEAD_DIM))
        return carry

    lax.fori_loop(0, heads, state_body, 0)

    for turn, by in enumerate(shifts):
        copies = [
            pltpu.make_async_remote_copy(
                src_ref=source.at[turn],
                dst_ref=target.at[turn],
                send_sem=sems.at[0, turn],
                recv_sem=sems.at[1, turn],
                device_id=at(place + by),
                device_id_type=MESH_ID,
            )
            for source, target, sems in (
                (state_out, state_in, state_sems),
                (total_out, total_in, total_sems),
            )
        ]

        @pl.when(place + by < sp_size)
        def _():
            for copy in copies:
                copy.start()

        if late < pieces:
            send_weight(0, 1, late)
            late += 1
        if turn == 0:

            @pl.when(place == 0)
            def _():
                carried[...] = jnp.zeros_like(carried)
                span_total[...] = jnp.zeros_like(span_total)

        @pl.when(place - by >= 0)
        def _():
            for copy in copies:
                copy.wait_recv()

            def merge(head, carry):
                arrived = state_in[turn, head].astype(jnp.float32)
                passed = total_in[turn, head]
                if turn == 0:
                    carried[head] = arrived
                    span_total[head] = passed
                else:
                    carried[head] = arrived * jnp.exp(span_total[head, 0:1, :]) + carried[head]
                    span_total[head] = span_total[head] + passed
                return carry

            lax.fori_loop(0, heads, merge, 0)

        if turn + 1 < len(shifts):
            state_out[turn + 1] = carried[...].astype(jnp.bfloat16)
            total_out[turn + 1] = span_total[...]

    for piece in range(late, pieces):
        send_weight(0, 1, piece)
    if line > 1:
        take_hop(1)
    loads[3].wait()
    loads[4].wait()
    gain = gain_ref[...]

    def compute(head, put):
        head_output(
            lanes_of(head),
            head,
            rows,
            query_ref,
            forget_ref,
            value_ref,
            gate_ref,
            gap_ref,
            surge_ref,
            gain,
            carried[head],
            put,
        )

    def head_of(chunk, parity):
        return (chunk // per * 2 + parity) * per + chunk % per

    def columns(chunk):
        return pl.ds(pl.multiple_of(chunk * HEAD_DIM, HEAD_DIM), HEAD_DIM)

    def swap_copy(chunk):
        return pltpu.make_async_remote_copy(
            src_ref=away.at[:, columns(chunk)],
            dst_ref=parts_ref.at[1, tp, :, columns(chunk)],
            send_sem=swap_sems.at[0, chunk],
            recv_sem=swap_sems.at[1, chunk],
            device_id={"lo": 1 - lo},
            device_id_type=MESH_ID,
        )

    def tp_copy(stage, which, mine, chunk):
        slot = tp
        for bit, stride in enumerate(strides[:stage]):
            if (mine >> bit) & 1:
                slot = slot + stride - 2 * stride * ((tp // stride) % 2)
        return pltpu.make_async_remote_copy(
            src_ref=parts_ref.at[which, slot, :, columns(chunk)],
            dst_ref=parts_ref.at[which, slot, :, columns(chunk)],
            send_sem=tp_sems.at[0, stage, which, mine, chunk],
            recv_sem=tp_sems.at[1, stage, which, mine, chunk],
            device_id={"tp": flipped(strides[stage])},
            device_id_type=MESH_ID,
        )

    def away_body(chunk, carry):
        def put(span, value):
            away[span, columns(chunk)] = value

        compute(head_of(chunk, 1 - lo), put)
        swap_copy(chunk).start()
        return carry

    lax.fori_loop(0, half, away_body, 0)

    def own_body(chunk, carry):
        def put(span, value):
            parts_ref[0, tp, span, columns(chunk)] = value

        compute(head_of(chunk, lo), put)
        for stage in range(len(strides)):
            tp_copy(stage, 0, 0, chunk).start()
        swap_copy(chunk).wait_recv()
        for stage in range(len(strides)):
            tp_copy(stage, 1, 0, chunk).start()
        return carry

    lax.fori_loop(0, half, own_body, 0)

    if line > 2:
        take_hop(2)

    for stage in range(len(strides)):

        def pass_body(chunk, carry):
            for which in (0, 1):
                for mine in range(1 << stage):
                    tp_copy(stage, which, mine, chunk).wait_recv()
                    for later in range(stage + 1, len(strides)):
                        tp_copy(later, which, mine | (1 << stage), chunk).start()
            return carry

        lax.fori_loop(0, half, pass_body, 0)

    for hop in range(3, line - 1):
        take_hop(hop)

    def partial_copy(piece):
        return pltpu.make_async_remote_copy(
            src_ref=partial_out.at[piece],
            dst_ref=partial_in.at[piece],
            send_sem=partial_sems.at[0, piece],
            recv_sem=partial_sems.at[1, piece],
            device_id={"lo": 1 - lo},
            device_id_type=MESH_ID,
        )

    def multiplied(which, piece):
        part_width = width // 2
        total = None
        for place in range(tp_size):
            block = whole_weight[pl.ds(place * part_width, part_width), pl.ds(piece * tile, tile)]
            term = dot(parts_ref[which, place], block)
            total = term if total is None else total + term
        return total

    for piece in range(pieces):
        if line > 3:
            take_weight(line - 1, piece)
        partial_out[piece] = multiplied(1, piece).astype(jnp.bfloat16)
        partial_copy(piece).start()
        here[piece] = multiplied(0, piece)
    for piece in range(pieces):
        partial_copy(piece).wait_recv()
        total = here[piece] + partial_in[piece].astype(jnp.float32)
        projected_ref[:, pl.ds(piece * tile, tile)] = total.astype(jnp.bfloat16)

    for piece in range(pieces):
        partial_copy(piece).wait_send()
        for way in (0, 1):
            for hop in range(1, line):

                @pl.when(sends(way, hop))
                def _():
                    weight_copy(way, hop, piece).wait_send()

    for turn, by in enumerate(shifts):

        @pl.when(place + by < sp_size)
        def _():
            for source, target, sems in (
                (state_out, state_in, state_sems),
                (total_out, total_in, total_sems),
            ):
                pltpu.make_async_remote_copy(
                    src_ref=source.at[turn],
                    dst_ref=target.at[turn],
                    send_sem=sems.at[0, turn],
                    recv_sem=sems.at[1, turn],
                    device_id=at(place + by),
                    device_id_type=MESH_ID,
                ).wait_send()

    def sent_body(chunk, carry):
        swap_copy(chunk).wait_send()
        for stage in range(len(strides)):
            for which in (0, 1):
                for mine in range(1 << stage):
                    tp_copy(stage, which, mine, chunk).wait_send()
        return carry

    lax.fori_loop(0, half, sent_body, 0)


def front(
    sizes, query_logits, forget_logits, value_inputs, gate_logits, gap, surge, gain, weight
):
    hi_size, inner_size, tp_size, block = sizes
    rows, width = query_logits.shape
    heads = width // HEAD_DIM
    turns = 1 + (2 * hi_size * inner_size - 2).bit_length()
    stages = tp_size.bit_length() - 1
    vmem = pl.BlockSpec(memory_space=pltpu.VMEM)
    anywhere = pl.BlockSpec(memory_space=pl.ANY)
    state = (heads, HEAD_DIM, HEAD_DIM)
    line = hi_size * inner_size
    depth, columns = weight.shape
    tile = 256
    pieces = columns // tile
    return pl.pallas_call(
        functools.partial(front_kernel, sizes),
        in_specs=[anywhere] * 4 + [vmem] * 3 + [anywhere],
        out_specs=vmem,
        out_shape=jax.ShapeDtypeStruct((rows, columns), jnp.bfloat16),
        scratch_shapes=[
            pltpu.VMEM((2, tp_size, rows, width // 2), jnp.bfloat16),
            pltpu.VMEM((line * depth, columns), jnp.bfloat16),
            pltpu.VMEM((turns,) + state, jnp.bfloat16),
            pltpu.VMEM((turns, heads, 8, HEAD_DIM), jnp.float32),
            pltpu.VMEM((turns,) + state, jnp.bfloat16),
            pltpu.VMEM((turns, heads, 8, HEAD_DIM), jnp.float32),
            pltpu.VMEM(state, jnp.float32),
            pltpu.VMEM((heads, 8, HEAD_DIM), jnp.float32),
            pltpu.VMEM((rows, width // 2), jnp.bfloat16),
            pltpu.VMEM((rows, width), jnp.bfloat16),
            pltpu.VMEM((rows, width), jnp.bfloat16),
            pltpu.VMEM((rows, width), jnp.bfloat16),
            pltpu.VMEM((rows, width), jnp.bfloat16),
            pltpu.VMEM((pieces, rows, tile), jnp.bfloat16),
            pltpu.VMEM((pieces, rows, tile), jnp.bfloat16),
            pltpu.VMEM((pieces, rows, tile), jnp.float32),
            pltpu.SemaphoreType.DMA((2, turns)),
            pltpu.SemaphoreType.DMA((2, turns)),
            pltpu.SemaphoreType.DMA((2, heads // 2)),
            pltpu.SemaphoreType.DMA((2, stages, 2, tp_size // 2, heads // 2)),
            pltpu.SemaphoreType.DMA((5,)),
            pltpu.SemaphoreType.DMA((2, 2, max(1, line - 1), pieces)),
            pltpu.SemaphoreType.DMA((2, pieces)),
        ],
        name="front",
        compiler_params=pltpu.CompilerParams(
            collective_id=0, has_side_effects=True, vmem_limit_bytes=48 * 1024 * 1024
        ),
        cost_estimate=pl.CostEstimate(
            flops=rows * width * 2000, bytes_accessed=8 * rows * width, transcendentals=0
        ),
    )(query_logits, forget_logits, value_inputs, gate_logits, gap, surge, gain, weight)


def per_device(
    hi_size,
    inner_size,
    tp_size,
    query_logits,
    forget_logits,
    value_inputs,
    output_gate_logits,
    forget_floor_gap,
    surge_log_decay,
    head_norm_gain,
    output_matrix,
    branch_norm_gain,
    residual,
):
    rows, width = query_logits.shape
    heads = width // HEAD_DIM
    column = lax.axis_index("tp")
    gap = lax.dynamic_slice_in_dim(
        forget_floor_gap.reshape(-1, 1, HEAD_DIM), column * heads, heads, axis=0
    )
    projected = front(
        (hi_size, inner_size, tp_size, inner_size * output_matrix.shape[0]),
        query_logits,
        forget_logits,
        value_inputs,
        output_gate_logits,
        gap,
        surge_log_decay.reshape(heads, 1, rows),
        head_norm_gain.reshape(1, HEAD_DIM),
        output_matrix,
    )
    branch = lax.optimization_barrier(projected).astype(jnp.float32)
    squares = lax.psum(jnp.sum(branch * branch, axis=1), "tp")
    columns = branch.shape[1]
    scale = lax.rsqrt(squares / (columns * tp_size) + EPSILON)
    gain_part = lax.dynamic_slice_in_dim(branch_norm_gain, column * columns, columns)
    return (residual.astype(jnp.float32) + branch * scale[:, None] * gain_part).astype(jnp.bfloat16)


def solution(mesh):
    sp_size, tp_size = mesh.shape["sp"], mesh.shape["tp"]
    sp = ("hi", "lo", "inner")
    placed = (
        P(sp, "tp"),
        P(sp, "tp"),
        P(sp, "tp"),
        P(sp, "tp"),
        P(),
        P("tp", sp),
        P(),
        P(sp, "tp"),
        P(),
        P(sp, "tp"),
    )

    def whole(*arrays):
        inner = max(1, HEAD_DIM * sp_size // arrays[7].shape[0])
        hi = sp_size // (2 * inner)
        devices = mesh.devices.reshape(hi, 2, inner, tp_size)
        paired = Mesh(devices, ("hi", "lo", "inner", "tp"))
        return jax.shard_map(
            functools.partial(per_device, hi, inner, tp_size),
            mesh=paired,
            in_specs=placed,
            out_specs=P(sp, "tp"),
            check_vma=False,
        )(*arrays)

    return whole
```

```python
import functools

import jax
import jax.numpy as jnp
from jax import lax
from jax.experimental import pallas as pl
from jax.experimental.pallas import tpu as pltpu
from jax.sharding import Mesh
from jax.sharding import PartitionSpec as P

HEAD_DIM = 128
SPAN = 128
EPSILON = 1e-06
NT = (((1,), (1,)), ((), ()))
TN = (((0,), (0,)), ((), ()))
NN = (((1,), (0,)), ((), ()))


def dot(a, b, dims=NN):
    return lax.dot_general(a, b, dims, preferred_element_type=jnp.float32)


def lower_triangle():
    rows = lax.broadcasted_iota(jnp.int32, (SPAN, SPAN), 0)
    columns = lax.broadcasted_iota(jnp.int32, (SPAN, SPAN), 1)
    return rows >= columns


def decays(logits, gap, surge, causal):
    keys = gap / (1.0 + jnp.exp(logits.astype(jnp.float32)))
    series = keys * (1.0 / 7.0) + (1.0 / 6.0)
    for order in (5, 4, 3, 2):
        series = series * keys + (1.0 / order)
    logs = -(series * keys + 1.0) * keys
    high = logs.astype(jnp.bfloat16)
    low = (logs - high.astype(jnp.float32)).astype(jnp.bfloat16)
    ones = causal.astype(jnp.bfloat16)
    surged = jnp.sum(jnp.where(causal, surge, 0.0), axis=1, keepdims=True)
    return keys, dot(ones, high) + dot(ones, low) + surged


def head_state(lanes, head, rows, forget_ref, value_ref, gap_ref, surge_ref):
    causal = lower_triangle()
    gap = gap_ref[head]
    state = jnp.zeros((HEAD_DIM, HEAD_DIM), jnp.float32)
    total = jnp.zeros((1, HEAD_DIM), jnp.float32)
    for start in range(0, rows, SPAN):
        span = pl.ds(start, SPAN)
        keys, running = decays(forget_ref[span, lanes], gap, surge_ref[head, :, span], causal)
        ending = running[SPAN - 1 : SPAN, :]
        kept = (keys * jnp.exp(ending - running)).astype(jnp.bfloat16)
        state = state * jnp.exp(ending) + dot(value_ref[span, lanes], kept, TN)
        total = total + ending
    return state, total


def head_output(
    lanes, head, rows, query_ref, forget_ref, value_ref, gate_ref, gap_ref, surge_ref, gain, state, put
):
    causal = lower_triangle()
    gap = gap_ref[head]
    middle = SPAN // 2
    for start in range(0, rows, SPAN):
        span = pl.ds(start, SPAN)
        keys, running = decays(forget_ref[span, lanes], gap, surge_ref[head, :, span], causal)
        anchor = running[middle - 1 : middle, :]
        ending = running[SPAN - 1 : SPAN, :]
        logits = query_ref[span, lanes].astype(jnp.float32)
        queries = logits * (HEAD_DIM**-0.5) / (1.0 + jnp.exp(-logits))
        reach = queries * jnp.exp(running - anchor)
        back = keys * jnp.exp(anchor - running)
        values = value_ref[span, lanes]
        scores = dot(reach.astype(jnp.bfloat16), back.astype(jnp.bfloat16), NT)
        scores = jnp.where(causal, scores, 0.0).astype(jnp.bfloat16)
        inter = dot(
            (reach * jnp.exp(anchor)).astype(jnp.bfloat16), state.astype(jnp.bfloat16), NT
        )
        out = inter + dot(scores, values)
        if start + SPAN < rows:
            kept = (back * jnp.exp(ending - anchor)).astype(jnp.bfloat16)
            state = state * jnp.exp(ending) + dot(values, kept, TN)
        mean_sq = jnp.mean(out * out, axis=1, keepdims=True)
        gates = gate_ref[span, lanes].astype(jnp.float32)
        gates = gates / (1.0 + jnp.exp(-gates))
        put(span, (out * lax.rsqrt(mean_sq + EPSILON) * gain * gates).astype(jnp.bfloat16))


MESH_ID = pl.DeviceIdType.MESH


def front_kernel(
    sizes,
    query_in,
    forget_in,
    value_in,
    gate_in,
    gap_ref,
    surge_ref,
    gain_ref,
    weight_ref,
    projected_ref,
    parts_ref,
    whole_weight,
    state_out,
    total_out,
    state_in,
    total_in,
    carried,
    span_total,
    away,
    query_ref,
    forget_ref,
    value_ref,
    gate_ref,
    partial_out,
    partial_in,
    here,
    state_sems,
    total_sems,
    swap_sems,
    tp_sems,
    load_sems,
    weight_sems,
    partial_sems,
):
    hi_size, inner_size, tp_size, block = sizes
    sp_size = 2 * hi_size * inner_size
    rows, width = query_in.shape
    heads = width // HEAD_DIM
    half = heads // 2
    per = block // HEAD_DIM
    lo, inner, tp = (lax.axis_index(a) for a in ("lo", "inner", "tp"))
    place = (lax.axis_index("hi") * 2 + lo) * inner_size + inner

    def at(position):
        return {
            "hi": position // (2 * inner_size),
            "lo": (position // inner_size) % 2,
            "inner": position % inner_size,
        }

    shifts = [1]
    by = 1
    while by < sp_size - 1:
        shifts.append(by)
        by *= 2
    strides = []
    stride = tp_size // 2
    while stride >= 1:
        strides.append(stride)
        stride //= 2

    def flipped(stride):
        return tp + stride - 2 * stride * ((tp // stride) % 2)

    line = hi_size * inner_size
    spot = lax.axis_index("hi") * inner_size + inner
    depth = weight_ref.shape[0]
    pieces, _, tile = partial_out.shape

    def slot(number):
        return pl.ds(pl.multiple_of(number * depth, depth), depth)

    loads = [
        pltpu.make_async_copy(source, target, load_sems.at[number])
        for number, (source, target) in enumerate(
            (
                (weight_ref, whole_weight.at[slot(spot)]),
                (forget_in, forget_ref),
                (value_in, value_ref),
                (query_in, query_ref),
                (gate_in, gate_ref),
            )
        )
    ]
    for load in loads:
        load.start()

    def on_line(position):
        return {"hi": position // inner_size, "inner": position % inner_size}

    def weight_copy(way, hop, piece):
        step = 1 if way == 0 else -1
        block = whole_weight.at[slot(spot - step * (hop - 1)), pl.ds(pl.multiple_of(piece * tile, tile), tile)]
        return pltpu.make_async_remote_copy(
            src_ref=block,
            dst_ref=block,
            send_sem=weight_sems.at[0, way, hop - 1, piece],
            recv_sem=weight_sems.at[1, way, hop - 1, piece],
            device_id=on_line(spot + step),
            device_id_type=MESH_ID,
        )

    def sends(way, hop):
        step = 1 if way == 0 else -1
        origin = spot - step * (hop - 1)
        target = spot + step
        return (origin >= 0) & (origin < line) & (target >= 0) & (target < line)

    def receives(way, hop):
        origin = spot - (1 if way == 0 else -1) * hop
        return (origin >= 0) & (origin < line)

    def send_weight(way, hop, piece):
        @pl.when(sends(way, hop))
        def _():
            weight_copy(way, hop, piece).start()

    def take_weight(hop, piece):
        for way in (0, 1):

            @pl.when(receives(way, hop))
            def _():
                weight_copy(way, hop, piece).wait_recv()

            if hop + 1 < line:
                send_weight(way, hop + 1, piece)

    def take_hop(hop):
        for piece in range(pieces):
            take_weight(hop, piece)

    barrier = pltpu.get_barrier_semaphore()
    reaches = sorted(set(shifts + [inner_size]))
    neighbours = [spot + 1, spot - 1]
    peers = len(strides)
    for by in reaches:
        for there in (place + by, place - by):
            inside = (there >= 0) & (there < sp_size)

            @pl.when(inside)
            def _():
                pl.semaphore_signal(barrier, inc=1, device_id=at(there), device_id_type=MESH_ID)

            peers = peers + jnp.where(inside, 1, 0)
    for there in neighbours:
        inside = (there >= 0) & (there < line)

        @pl.when(inside)
        def _():
            pl.semaphore_signal(barrier, inc=1, device_id=on_line(there), device_id_type=MESH_ID)

        peers = peers + jnp.where(inside, 1, 0)
    for stride in strides:
        pl.semaphore_signal(
            barrier, inc=1, device_id={"tp": flipped(stride)}, device_id_type=MESH_ID
        )
    pl.semaphore_wait(barrier, peers)
    loads[0].wait()
    late = pieces // 2
    for piece in range(pieces):
        send_weight(1, 1, piece)
        if piece < late:
            send_weight(0, 1, piece)
    loads[1].wait()
    loads[2].wait()

    def lanes_of(head):
        return pl.ds(pl.multiple_of(head * HEAD_DIM, HEAD_DIM), HEAD_DIM)

    def state_body(head, carry):
        state, total = head_state(
            lanes_of(head), head, rows, forget_ref, value_ref, gap_ref, surge_ref
        )
        state_out[0, head] = state.astype(jnp.bfloat16)
        total_out[0, head] = jnp.broadcast_to(total, (8, HEAD_DIM))
        return carry

    lax.fori_loop(0, heads, state_body, 0)

    hop_pieces_left = list(range(pieces))

    for turn, by in enumerate(shifts):
        copies = [
            pltpu.make_async_remote_copy(
                src_ref=source.at[turn],
                dst_ref=target.at[turn],
                send_sem=sems.at[0, turn],
                recv_sem=sems.at[1, turn],
                device_id=at(place + by),
                device_id_type=MESH_ID,
            )
            for source, target, sems in (
                (state_out, state_in, state_sems),
                (total_out, total_in, total_sems),
            )
        ]

        @pl.when(place + by < sp_size)
        def _():
            for copy in copies:
                copy.start()

        if late < pieces:
            send_weight(0, 1, late)
            late += 1
        if turn == 0:

            @pl.when(place == 0)
            def _():
                carried[...] = jnp.zeros_like(carried)
                span_total[...] = jnp.zeros_like(span_total)

        @pl.when(place - by >= 0)
        def _():
            for copy in copies:
                copy.wait_recv()

            def merge(head, carry):
                arrived = state_in[turn, head].astype(jnp.float32)
                passed = total_in[turn, head]
                if turn == 0:
                    carried[head] = arrived
                    span_total[head] = passed
                else:
                    carried[head] = arrived * jnp.exp(span_total[head, 0:1, :]) + carried[head]
                    span_total[head] = span_total[head] + passed
                return carry

            lax.fori_loop(0, heads, merge, 0)

        if line > 1 and turn < pieces:
            if turn + 1 < len(shifts):
                state_out[turn + 1] = carried[...].astype(jnp.bfloat16)
                total_out[turn + 1] = span_total[...]
            hop_pieces_left.remove(turn)
            take_weight(1, turn)
        elif turn + 1 < len(shifts):
            state_out[turn + 1] = carried[...].astype(jnp.bfloat16)
            total_out[turn + 1] = span_total[...]

    for piece in range(late, pieces):
        send_weight(0, 1, piece)
    if line > 1:
        for piece in hop_pieces_left:
            take_weight(1, piece)
    loads[3].wait()
    loads[4].wait()
    gain = gain_ref[...]

    def compute(head, put):
        head_output(
            lanes_of(head),
            head,
            rows,
            query_ref,
            forget_ref,
            value_ref,
            gate_ref,
            gap_ref,
            surge_ref,
            gain,
            carried[head],
            put,
        )

    def head_of(chunk, parity):
        return (chunk // per * 2 + parity) * per + chunk % per

    def columns(chunk):
        return pl.ds(pl.multiple_of(chunk * HEAD_DIM, HEAD_DIM), HEAD_DIM)

    def swap_copy(chunk):
        return pltpu.make_async_remote_copy(
            src_ref=away.at[:, columns(chunk)],
            dst_ref=parts_ref.at[1, tp, :, columns(chunk)],
            send_sem=swap_sems.at[0, chunk],
            recv_sem=swap_sems.at[1, chunk],
            device_id={"lo": 1 - lo},
            device_id_type=MESH_ID,
        )

    def tp_copy(stage, which, mine, chunk):
        slot = tp
        for bit, stride in enumerate(strides[:stage]):
            if (mine >> bit) & 1:
                slot = slot + stride - 2 * stride * ((tp // stride) % 2)
        return pltpu.make_async_remote_copy(
            src_ref=parts_ref.at[which, slot, :, columns(chunk)],
            dst_ref=parts_ref.at[which, slot, :, columns(chunk)],
            send_sem=tp_sems.at[0, stage, which, mine, chunk],
            recv_sem=tp_sems.at[1, stage, which, mine, chunk],
            device_id={"tp": flipped(strides[stage])},
            device_id_type=MESH_ID,
        )

    def away_body(chunk, carry):
        def put(span, value):
            away[span, columns(chunk)] = value

        compute(head_of(chunk, 1 - lo), put)
        swap_copy(chunk).start()
        if line > 2 and pieces == half:
            take_weight(2, chunk)
        return carry

    lax.fori_loop(0, half, away_body, 0)

    def own_body(chunk, carry):
        def put(span, value):
            parts_ref[0, tp, span, columns(chunk)] = value

        compute(head_of(chunk, lo), put)
        for stage in range(len(strides)):
            tp_copy(stage, 0, 0, chunk).start()
        swap_copy(chunk).wait_recv()
        for stage in range(len(strides)):
            tp_copy(stage, 1, 0, chunk).start()
        return carry

    lax.fori_loop(0, half, own_body, 0)

    if line > 2 and pieces != half:
        take_hop(2)

    for stage in range(len(strides)):

        def pass_body(chunk, carry):
            for which in (0, 1):
                for mine in range(1 << stage):
                    tp_copy(stage, which, mine, chunk).wait_recv()
                    for later in range(stage + 1, len(strides)):
                        tp_copy(later, which, mine | (1 << stage), chunk).start()
            return carry

        lax.fori_loop(0, half, pass_body, 0)

    for hop in range(3, line - 1):
        take_hop(hop)

    def partial_copy(piece):
        return pltpu.make_async_remote_copy(
            src_ref=partial_out.at[piece],
            dst_ref=partial_in.at[piece],
            send_sem=partial_sems.at[0, piece],
            recv_sem=partial_sems.at[1, piece],
            device_id={"lo": 1 - lo},
            device_id_type=MESH_ID,
        )

    def multiplied(which, piece):
        part_width = width // 2
        total = None
        for place in range(tp_size):
            block = whole_weight[pl.ds(place * part_width, part_width), pl.ds(piece * tile, tile)]
            term = dot(parts_ref[which, place], block)
            total = term if total is None else total + term
        return total

    for piece in range(pieces):
        if line > 3:
            take_weight(line - 1, piece)
        partial_out[piece] = multiplied(1, piece).astype(jnp.bfloat16)
        partial_copy(piece).start()
        here[piece] = multiplied(0, piece)
    for piece in range(pieces):
        partial_copy(piece).wait_recv()
        total = here[piece] + partial_in[piece].astype(jnp.float32)
        projected_ref[:, pl.ds(piece * tile, tile)] = total.astype(jnp.bfloat16)

    for piece in range(pieces):
        partial_copy(piece).wait_send()
        for way in (0, 1):
            for hop in range(1, line):

                @pl.when(sends(way, hop))
                def _():
                    weight_copy(way, hop, piece).wait_send()

    for turn, by in enumerate(shifts):

        @pl.when(place + by < sp_size)
        def _():
            for source, target, sems in (
                (state_out, state_in, state_sems),
                (total_out, total_in, total_sems),
            ):
                pltpu.make_async_remote_copy(
                    src_ref=source.at[turn],
                    dst_ref=target.at[turn],
                    send_sem=sems.at[0, turn],
                    recv_sem=sems.at[1, turn],
                    device_id=at(place + by),
                    device_id_type=MESH_ID,
                ).wait_send()

    def sent_body(chunk, carry):
        swap_copy(chunk).wait_send()
        for stage in range(len(strides)):
            for which in (0, 1):
                for mine in range(1 << stage):
                    tp_copy(stage, which, mine, chunk).wait_send()
        return carry

    lax.fori_loop(0, half, sent_body, 0)


def front(
    sizes, query_logits, forget_logits, value_inputs, gate_logits, gap, surge, gain, weight
):
    hi_size, inner_size, tp_size, block = sizes
    rows, width = query_logits.shape
    heads = width // HEAD_DIM
    turns = 1 + (2 * hi_size * inner_size - 2).bit_length()
    stages = tp_size.bit_length() - 1
    vmem = pl.BlockSpec(memory_space=pltpu.VMEM)
    anywhere = pl.BlockSpec(memory_space=pl.ANY)
    state = (heads, HEAD_DIM, HEAD_DIM)
    line = hi_size * inner_size
    depth, columns = weight.shape
    tile = 256
    pieces = columns // tile
    return pl.pallas_call(
        functools.partial(front_kernel, sizes),
        in_specs=[anywhere] * 4 + [vmem] * 3 + [anywhere],
        out_specs=vmem,
        out_shape=jax.ShapeDtypeStruct((rows, columns), jnp.bfloat16),
        scratch_shapes=[
            pltpu.VMEM((2, tp_size, rows, width // 2), jnp.bfloat16),
            pltpu.VMEM((line * depth, columns), jnp.bfloat16),
            pltpu.VMEM((turns,) + state, jnp.bfloat16),
            pltpu.VMEM((turns, heads, 8, HEAD_DIM), jnp.float32),
            pltpu.VMEM((turns,) + state, jnp.bfloat16),
            pltpu.VMEM((turns, heads, 8, HEAD_DIM), jnp.float32),
            pltpu.VMEM(state, jnp.float32),
            pltpu.VMEM((heads, 8, HEAD_DIM), jnp.float32),
            pltpu.VMEM((rows, width // 2), jnp.bfloat16),
            pltpu.VMEM((rows, width), jnp.bfloat16),
            pltpu.VMEM((rows, width), jnp.bfloat16),
            pltpu.VMEM((rows, width), jnp.bfloat16),
            pltpu.VMEM((rows, width), jnp.bfloat16),
            pltpu.VMEM((pieces, rows, tile), jnp.bfloat16),
            pltpu.VMEM((pieces, rows, tile), jnp.bfloat16),
            pltpu.VMEM((pieces, rows, tile), jnp.float32),
            pltpu.SemaphoreType.DMA((2, turns)),
            pltpu.SemaphoreType.DMA((2, turns)),
            pltpu.SemaphoreType.DMA((2, heads // 2)),
            pltpu.SemaphoreType.DMA((2, stages, 2, tp_size // 2, heads // 2)),
            pltpu.SemaphoreType.DMA((5,)),
            pltpu.SemaphoreType.DMA((2, 2, max(1, line - 1), pieces)),
            pltpu.SemaphoreType.DMA((2, pieces)),
        ],
        name="front",
        compiler_params=pltpu.CompilerParams(
            collective_id=0, has_side_effects=True, vmem_limit_bytes=64000 * 1024
        ),
        cost_estimate=pl.CostEstimate(
            flops=rows * width * 2000, bytes_accessed=8 * rows * width, transcendentals=0
        ),
    )(query_logits, forget_logits, value_inputs, gate_logits, gap, surge, gain, weight)


def per_device(
    hi_size,
    inner_size,
    tp_size,
    query_logits,
    forget_logits,
    value_inputs,
    output_gate_logits,
    forget_floor_gap,
    surge_log_decay,
    head_norm_gain,
    output_matrix,
    branch_norm_gain,
    residual,
):
    rows, width = query_logits.shape
    heads = width // HEAD_DIM
    column = lax.axis_index("tp")
    gap = lax.dynamic_slice_in_dim(
        forget_floor_gap.reshape(-1, 1, HEAD_DIM), column * heads, heads, axis=0
    )
    projected = front(
        (hi_size, inner_size, tp_size, inner_size * output_matrix.shape[0]),
        query_logits,
        forget_logits,
        value_inputs,
        output_gate_logits,
        gap,
        surge_log_decay.reshape(heads, 1, rows),
        head_norm_gain.reshape(1, HEAD_DIM),
        output_matrix,
    )
    branch = lax.optimization_barrier(projected).astype(jnp.float32)
    squares = lax.psum(jnp.sum(branch * branch, axis=1), "tp")
    columns = branch.shape[1]
    scale = lax.rsqrt(squares / (columns * tp_size) + EPSILON)
    gain_part = lax.dynamic_slice_in_dim(branch_norm_gain, column * columns, columns)
    return (residual.astype(jnp.float32) + branch * scale[:, None] * gain_part).astype(jnp.bfloat16)


def solution(mesh):
    sp_size, tp_size = mesh.shape["sp"], mesh.shape["tp"]
    sp = ("hi", "lo", "inner")
    placed = (
        P(sp, "tp"),
        P(sp, "tp"),
        P(sp, "tp"),
        P(sp, "tp"),
        P(),
        P("tp", sp),
        P(),
        P(sp, "tp"),
        P(),
        P(sp, "tp"),
    )

    def whole(*arrays):
        inner = max(1, HEAD_DIM * sp_size // arrays[7].shape[0])
        hi = sp_size // (2 * inner)
        devices = mesh.devices.reshape(hi, 2, inner, tp_size)
        paired = Mesh(devices, ("hi", "lo", "inner", "tp"))
        return jax.shard_map(
            functools.partial(per_device, hi, inner, tp_size),
            mesh=paired,
            in_specs=placed,
            out_specs=P(sp, "tp"),
            check_vma=False,
        )(*arrays)

    return whole
```

```python
import functools

import jax
import jax.numpy as jnp
from jax import lax
from jax.experimental import pallas as pl
from jax.experimental.pallas import tpu as pltpu
from jax.sharding import Mesh
from jax.sharding import PartitionSpec as P

HEAD_DIM = 128
SPAN = 128
EPSILON = 1e-06
NT = (((1,), (1,)), ((), ()))
TN = (((0,), (0,)), ((), ()))
NN = (((1,), (0,)), ((), ()))


def dot(a, b, dims=NN):
    return lax.dot_general(a, b, dims, preferred_element_type=jnp.float32)


def lower_triangle():
    rows = lax.broadcasted_iota(jnp.int32, (SPAN, SPAN), 0)
    columns = lax.broadcasted_iota(jnp.int32, (SPAN, SPAN), 1)
    return rows >= columns


def decays(logits, gap, surge, causal):
    keys = gap / (1.0 + jnp.exp(logits.astype(jnp.float32)))
    series = keys * (1.0 / 7.0) + (1.0 / 6.0)
    for order in (5, 4, 3, 2):
        series = series * keys + (1.0 / order)
    logs = -(series * keys + 1.0) * keys
    high = logs.astype(jnp.bfloat16)
    low = (logs - high.astype(jnp.float32)).astype(jnp.bfloat16)
    ones = causal.astype(jnp.bfloat16)
    surged = jnp.sum(jnp.where(causal, surge, 0.0), axis=1, keepdims=True)
    return keys, dot(ones, high) + dot(ones, low) + surged


def head_state(lanes, head, rows, forget_ref, value_ref, gap_ref, surge_ref):
    causal = lower_triangle()
    gap = gap_ref[head]
    state = jnp.zeros((HEAD_DIM, HEAD_DIM), jnp.float32)
    total = jnp.zeros((1, HEAD_DIM), jnp.float32)
    for start in range(0, rows, SPAN):
        span = pl.ds(start, SPAN)
        keys, running = decays(forget_ref[span, lanes], gap, surge_ref[head, :, span], causal)
        ending = running[SPAN - 1 : SPAN, :]
        kept = (keys * jnp.exp(ending - running)).astype(jnp.bfloat16)
        state = state * jnp.exp(ending) + dot(value_ref[span, lanes], kept, TN)
        total = total + ending
    return state, total


def head_output(
    lanes, head, rows, query_ref, forget_ref, value_ref, gate_ref, gap_ref, surge_ref, gain, state, put
):
    causal = lower_triangle()
    gap = gap_ref[head]
    middle = SPAN // 2
    for start in range(0, rows, SPAN):
        span = pl.ds(start, SPAN)
        keys, running = decays(forget_ref[span, lanes], gap, surge_ref[head, :, span], causal)
        anchor = running[middle - 1 : middle, :]
        ending = running[SPAN - 1 : SPAN, :]
        logits = query_ref[span, lanes].astype(jnp.float32)
        queries = logits * (HEAD_DIM**-0.5) / (1.0 + jnp.exp(-logits))
        reach = queries * jnp.exp(running - anchor)
        back = keys * jnp.exp(anchor - running)
        values = value_ref[span, lanes]
        scores = dot(reach.astype(jnp.bfloat16), back.astype(jnp.bfloat16), NT)
        scores = jnp.where(causal, scores, 0.0).astype(jnp.bfloat16)
        inter = dot(
            (reach * jnp.exp(anchor)).astype(jnp.bfloat16), state.astype(jnp.bfloat16), NT
        )
        out = inter + dot(scores, values)
        if start + SPAN < rows:
            kept = (back * jnp.exp(ending - anchor)).astype(jnp.bfloat16)
            state = state * jnp.exp(ending) + dot(values, kept, TN)
        mean_sq = jnp.mean(out * out, axis=1, keepdims=True)
        gates = gate_ref[span, lanes].astype(jnp.float32)
        gates = gates / (1.0 + jnp.exp(-gates))
        put(span, (out * lax.rsqrt(mean_sq + EPSILON) * gain * gates).astype(jnp.bfloat16))


MESH_ID = pl.DeviceIdType.MESH


def front_kernel(
    sizes,
    query_in,
    forget_in,
    value_in,
    gate_in,
    gap_ref,
    surge_ref,
    gain_ref,
    weight_ref,
    projected_ref,
    parts_ref,
    whole_weight,
    state_out,
    total_out,
    state_in,
    total_in,
    carried,
    span_total,
    away,
    query_ref,
    forget_ref,
    value_ref,
    gate_ref,
    partial_out,
    partial_in,
    here,
    state_sems,
    total_sems,
    swap_sems,
    tp_sems,
    load_sems,
    weight_sems,
    partial_sems,
):
    hi_size, inner_size, tp_size, block = sizes
    sp_size = 2 * hi_size * inner_size
    rows, width = query_in.shape
    heads = width // HEAD_DIM
    half = heads // 2
    per = block // HEAD_DIM
    lo, inner, tp = (lax.axis_index(a) for a in ("lo", "inner", "tp"))
    place = (lax.axis_index("hi") * 2 + lo) * inner_size + inner

    def at(position):
        return {
            "hi": position // (2 * inner_size),
            "lo": (position // inner_size) % 2,
            "inner": position % inner_size,
        }

    shifts = [1]
    passed_back = 0
    by = 1
    while by < sp_size - 1:
        shifts.append(by)
        by *= 2
    strides = []
    stride = tp_size // 2
    while stride >= 1:
        strides.append(stride)
        stride //= 2

    def flipped(stride):
        return tp + stride - 2 * stride * ((tp // stride) % 2)

    line = hi_size * inner_size
    spot = lax.axis_index("hi") * inner_size + inner
    depth = weight_ref.shape[0]
    pieces, _, tile = partial_out.shape

    def slot(number):
        return pl.ds(pl.multiple_of(number * depth, depth), depth)

    loads = [
        pltpu.make_async_copy(source, target, load_sems.at[number])
        for number, (source, target) in enumerate(
            (
                (weight_ref, whole_weight.at[slot(spot)]),
                (forget_in, forget_ref),
                (value_in, value_ref),
                (query_in, query_ref),
                (gate_in, gate_ref),
            )
        )
    ]
    for load in loads:
        load.start()

    def on_line(position):
        return {"hi": position // inner_size, "inner": position % inner_size}

    def weight_copy(way, hop, piece):
        step = 1 if way == 0 else -1
        block = whole_weight.at[slot(spot - step * (hop - 1)), pl.ds(pl.multiple_of(piece * tile, tile), tile)]
        return pltpu.make_async_remote_copy(
            src_ref=block,
            dst_ref=block,
            send_sem=weight_sems.at[0, way, hop - 1, piece],
            recv_sem=weight_sems.at[1, way, hop - 1, piece],
            device_id=on_line(spot + step),
            device_id_type=MESH_ID,
        )

    def sends(way, hop):
        step = 1 if way == 0 else -1
        origin = spot - step * (hop - 1)
        target = spot + step
        return (origin >= 0) & (origin < line) & (target >= 0) & (target < line)

    def receives(way, hop):
        origin = spot - (1 if way == 0 else -1) * hop
        return (origin >= 0) & (origin < line)

    def send_weight(way, hop, piece):
        @pl.when(sends(way, hop))
        def _():
            weight_copy(way, hop, piece).start()

    def take_weight(hop, piece, ways=(0, 1)):
        for way in ways:

            @pl.when(receives(way, hop))
            def _():
                weight_copy(way, hop, piece).wait_recv()

            if hop + 1 < line:
                send_weight(way, hop + 1, piece)

    def take_hop(hop):
        for piece in range(pieces):
            take_weight(hop, piece)

    barrier = pltpu.get_barrier_semaphore()
    reaches = sorted(set(shifts + [inner_size]))
    neighbours = [spot + 1, spot - 1]
    peers = len(strides)
    for by in reaches:
        for there in (place + by, place - by):
            inside = (there >= 0) & (there < sp_size)

            @pl.when(inside)
            def _():
                pl.semaphore_signal(barrier, inc=1, device_id=at(there), device_id_type=MESH_ID)

            peers = peers + jnp.where(inside, 1, 0)
    for there in neighbours:
        inside = (there >= 0) & (there < line)

        @pl.when(inside)
        def _():
            pl.semaphore_signal(barrier, inc=1, device_id=on_line(there), device_id_type=MESH_ID)

        peers = peers + jnp.where(inside, 1, 0)
    for stride in strides:
        pl.semaphore_signal(
            barrier, inc=1, device_id={"tp": flipped(stride)}, device_id_type=MESH_ID
        )
    pl.semaphore_wait(barrier, peers)
    loads[0].wait()
    late = pieces // 2
    for piece in range(pieces):
        send_weight(1, 1, piece)
        if piece < late:
            send_weight(0, 1, piece)
    loads[1].wait()
    loads[2].wait()

    def lanes_of(head):
        return pl.ds(pl.multiple_of(head * HEAD_DIM, HEAD_DIM), HEAD_DIM)

    def state_body(head, carry):
        state, total = head_state(
            lanes_of(head), head, rows, forget_ref, value_ref, gap_ref, surge_ref
        )
        state_out[0, head] = state.astype(jnp.bfloat16)
        total_out[0, head] = jnp.broadcast_to(total, (8, HEAD_DIM))
        return carry

    lax.fori_loop(0, heads, state_body, 0)

    for turn, by in enumerate(shifts):
        copies = [
            pltpu.make_async_remote_copy(
                src_ref=source.at[turn],
                dst_ref=target.at[turn],
                send_sem=sems.at[0, turn],
                recv_sem=sems.at[1, turn],
                device_id=at(place + by),
                device_id_type=MESH_ID,
            )
            for source, target, sems in (
                (state_out, state_in, state_sems),
                (total_out, total_in, total_sems),
            )
        ]

        @pl.when(place + by < sp_size)
        def _():
            for copy in copies:
                copy.start()

        if late < pieces:
            send_weight(0, 1, late)
            late += 1
        if turn == 0:

            @pl.when(place == 0)
            def _():
                carried[...] = jnp.zeros_like(carried)
                span_total[...] = jnp.zeros_like(span_total)

        @pl.when(place - by >= 0)
        def _():
            for copy in copies:
                copy.wait_recv()

            def merge(head, carry):
                arrived = state_in[turn, head].astype(jnp.float32)
                passed = total_in[turn, head]
                if turn == 0:
                    carried[head] = arrived
                    span_total[head] = passed
                else:
                    carried[head] = arrived * jnp.exp(span_total[head, 0:1, :]) + carried[head]
                    span_total[head] = span_total[head] + passed
                return carry

            lax.fori_loop(0, heads, merge, 0)

        if turn + 1 < len(shifts):
            state_out[turn + 1] = carried[...].astype(jnp.bfloat16)
            total_out[turn + 1] = span_total[...]
            if line > 1 and turn >= 1 and turn - 1 < pieces:
                take_weight(1, turn - 1, (1,))
                passed_back = turn

    for piece in range(late, pieces):
        send_weight(0, 1, piece)
    if line > 1:
        for piece in range(pieces):
            take_weight(1, piece, (0, 1) if piece >= passed_back else (0,))
    loads[3].wait()
    loads[4].wait()
    gain = gain_ref[...]

    def compute(head, put):
        head_output(
            lanes_of(head),
            head,
            rows,
            query_ref,
            forget_ref,
            value_ref,
            gate_ref,
            gap_ref,
            surge_ref,
            gain,
            carried[head],
            put,
        )

    def head_of(chunk, parity):
        return (chunk // per * 2 + parity) * per + chunk % per

    def columns(chunk):
        return pl.ds(pl.multiple_of(chunk * HEAD_DIM, HEAD_DIM), HEAD_DIM)

    def swap_copy(chunk):
        return pltpu.make_async_remote_copy(
            src_ref=away.at[:, columns(chunk)],
            dst_ref=parts_ref.at[1, tp, :, columns(chunk)],
            send_sem=swap_sems.at[0, chunk],
            recv_sem=swap_sems.at[1, chunk],
            device_id={"lo": 1 - lo},
            device_id_type=MESH_ID,
        )

    def tp_copy(stage, which, mine, chunk):
        slot = tp
        for bit, stride in enumerate(strides[:stage]):
            if (mine >> bit) & 1:
                slot = slot + stride - 2 * stride * ((tp // stride) % 2)
        return pltpu.make_async_remote_copy(
            src_ref=parts_ref.at[which, slot, :, columns(chunk)],
            dst_ref=parts_ref.at[which, slot, :, columns(chunk)],
            send_sem=tp_sems.at[0, stage, which, mine, chunk],
            recv_sem=tp_sems.at[1, stage, which, mine, chunk],
            device_id={"tp": flipped(strides[stage])},
            device_id_type=MESH_ID,
        )

    def away_body(chunk, carry):
        def put(span, value):
            away[span, columns(chunk)] = value

        compute(head_of(chunk, 1 - lo), put)
        swap_copy(chunk).start()
        if line > 2 and pieces == half:
            take_weight(2, chunk, (1,))
        return carry

    lax.fori_loop(0, half, away_body, 0)

    def own_body(chunk, carry):
        def put(span, value):
            parts_ref[0, tp, span, columns(chunk)] = value

        compute(head_of(chunk, lo), put)
        for stage in range(len(strides)):
            tp_copy(stage, 0, 0, chunk).start()
        swap_copy(chunk).wait_recv()
        for stage in range(len(strides)):
            tp_copy(stage, 1, 0, chunk).start()
        return carry

    lax.fori_loop(0, half, own_body, 0)

    if line > 2:
        for piece in range(pieces):
            take_weight(2, piece, (0,) if pieces == half else (0, 1))

    for stage in range(len(strides)):

        def pass_body(chunk, carry):
            for which in (0, 1):
                for mine in range(1 << stage):
                    tp_copy(stage, which, mine, chunk).wait_recv()
                    for later in range(stage + 1, len(strides)):
                        tp_copy(later, which, mine | (1 << stage), chunk).start()
            return carry

        lax.fori_loop(0, half, pass_body, 0)

    for hop in range(3, line - 1):
        take_hop(hop)

    def partial_copy(piece):
        return pltpu.make_async_remote_copy(
            src_ref=partial_out.at[piece],
            dst_ref=partial_in.at[piece],
            send_sem=partial_sems.at[0, piece],
            recv_sem=partial_sems.at[1, piece],
            device_id={"lo": 1 - lo},
            device_id_type=MESH_ID,
        )

    def multiplied(which, piece):
        part_width = width // 2
        total = None
        for place in range(tp_size):
            block = whole_weight[pl.ds(place * part_width, part_width), pl.ds(piece * tile, tile)]
            term = dot(parts_ref[which, place], block)
            total = term if total is None else total + term
        return total

    for piece in range(pieces):
        if line > 3:
            take_weight(line - 1, piece)
        partial_out[piece] = multiplied(1, piece).astype(jnp.bfloat16)
        partial_copy(piece).start()
        here[piece] = multiplied(0, piece)
    for piece in range(pieces):
        partial_copy(piece).wait_recv()
        total = here[piece] + partial_in[piece].astype(jnp.float32)
        projected_ref[:, pl.ds(piece * tile, tile)] = total.astype(jnp.bfloat16)

    for piece in range(pieces):
        partial_copy(piece).wait_send()
        for way in (0, 1):
            for hop in range(1, line):

                @pl.when(sends(way, hop))
                def _():
                    weight_copy(way, hop, piece).wait_send()

    for turn, by in enumerate(shifts):

        @pl.when(place + by < sp_size)
        def _():
            for source, target, sems in (
                (state_out, state_in, state_sems),
                (total_out, total_in, total_sems),
            ):
                pltpu.make_async_remote_copy(
                    src_ref=source.at[turn],
                    dst_ref=target.at[turn],
                    send_sem=sems.at[0, turn],
                    recv_sem=sems.at[1, turn],
                    device_id=at(place + by),
                    device_id_type=MESH_ID,
                ).wait_send()

    def sent_body(chunk, carry):
        swap_copy(chunk).wait_send()
        for stage in range(len(strides)):
            for which in (0, 1):
                for mine in range(1 << stage):
                    tp_copy(stage, which, mine, chunk).wait_send()
        return carry

    lax.fori_loop(0, half, sent_body, 0)


def front(
    sizes, query_logits, forget_logits, value_inputs, gate_logits, gap, surge, gain, weight
):
    hi_size, inner_size, tp_size, block = sizes
    rows, width = query_logits.shape
    heads = width // HEAD_DIM
    turns = 1 + (2 * hi_size * inner_size - 2).bit_length()
    stages = tp_size.bit_length() - 1
    vmem = pl.BlockSpec(memory_space=pltpu.VMEM)
    anywhere = pl.BlockSpec(memory_space=pl.ANY)
    state = (heads, HEAD_DIM, HEAD_DIM)
    line = hi_size * inner_size
    depth, columns = weight.shape
    tile = 256
    pieces = columns // tile
    return pl.pallas_call(
        functools.partial(front_kernel, sizes),
        in_specs=[anywhere] * 4 + [vmem] * 3 + [anywhere],
        out_specs=vmem,
        out_shape=jax.ShapeDtypeStruct((rows, columns), jnp.bfloat16),
        scratch_shapes=[
            pltpu.VMEM((2, tp_size, rows, width // 2), jnp.bfloat16),
            pltpu.VMEM((line * depth, columns), jnp.bfloat16),
            pltpu.VMEM((turns,) + state, jnp.bfloat16),
            pltpu.VMEM((turns, heads, 8, HEAD_DIM), jnp.float32),
            pltpu.VMEM((turns,) + state, jnp.bfloat16),
            pltpu.VMEM((turns, heads, 8, HEAD_DIM), jnp.float32),
            pltpu.VMEM(state, jnp.float32),
            pltpu.VMEM((heads, 8, HEAD_DIM), jnp.float32),
            pltpu.VMEM((rows, width // 2), jnp.bfloat16),
            pltpu.VMEM((rows, width), jnp.bfloat16),
            pltpu.VMEM((rows, width), jnp.bfloat16),
            pltpu.VMEM((rows, width), jnp.bfloat16),
            pltpu.VMEM((rows, width), jnp.bfloat16),
            pltpu.VMEM((pieces, rows, tile), jnp.bfloat16),
            pltpu.VMEM((pieces, rows, tile), jnp.bfloat16),
            pltpu.VMEM((pieces, rows, tile), jnp.float32),
            pltpu.SemaphoreType.DMA((2, turns)),
            pltpu.SemaphoreType.DMA((2, turns)),
            pltpu.SemaphoreType.DMA((2, heads // 2)),
            pltpu.SemaphoreType.DMA((2, stages, 2, tp_size // 2, heads // 2)),
            pltpu.SemaphoreType.DMA((5,)),
            pltpu.SemaphoreType.DMA((2, 2, max(1, line - 1), pieces)),
            pltpu.SemaphoreType.DMA((2, pieces)),
        ],
        name="front",
        compiler_params=pltpu.CompilerParams(
            collective_id=0, has_side_effects=True, vmem_limit_bytes=64000 * 1024
        ),
        cost_estimate=pl.CostEstimate(
            flops=rows * width * 2000, bytes_accessed=8 * rows * width, transcendentals=0
        ),
    )(query_logits, forget_logits, value_inputs, gate_logits, gap, surge, gain, weight)


def per_device(
    hi_size,
    inner_size,
    tp_size,
    query_logits,
    forget_logits,
    value_inputs,
    output_gate_logits,
    forget_floor_gap,
    surge_log_decay,
    head_norm_gain,
    output_matrix,
    branch_norm_gain,
    residual,
):
    rows, width = query_logits.shape
    heads = width // HEAD_DIM
    column = lax.axis_index("tp")
    gap = lax.dynamic_slice_in_dim(
        forget_floor_gap.reshape(-1, 1, HEAD_DIM), column * heads, heads, axis=0
    )
    projected = front(
        (hi_size, inner_size, tp_size, inner_size * output_matrix.shape[0]),
        query_logits,
        forget_logits,
        value_inputs,
        output_gate_logits,
        gap,
        surge_log_decay.reshape(heads, 1, rows),
        head_norm_gain.reshape(1, HEAD_DIM),
        output_matrix,
    )
    branch = lax.optimization_barrier(projected).astype(jnp.float32)
    squares = lax.psum(jnp.sum(branch * branch, axis=1), "tp")
    columns = branch.shape[1]
    scale = lax.rsqrt(squares / (columns * tp_size) + EPSILON)
    gain_part = lax.dynamic_slice_in_dim(branch_norm_gain, column * columns, columns)
    return (residual.astype(jnp.float32) + branch * scale[:, None] * gain_part).astype(jnp.bfloat16)


def solution(mesh):
    sp_size, tp_size = mesh.shape["sp"], mesh.shape["tp"]
    sp = ("hi", "lo", "inner")
    placed = (
        P(sp, "tp"),
        P(sp, "tp"),
        P(sp, "tp"),
        P(sp, "tp"),
        P(),
        P("tp", sp),
        P(),
        P(sp, "tp"),
        P(),
        P(sp, "tp"),
    )

    def whole(*arrays):
        inner = max(1, HEAD_DIM * sp_size // arrays[7].shape[0])
        hi = sp_size // (2 * inner)
        devices = mesh.devices.reshape(hi, 2, inner, tp_size)
        paired = Mesh(devices, ("hi", "lo", "inner", "tp"))
        return jax.shard_map(
            functools.partial(per_device, hi, inner, tp_size),
            mesh=paired,
            in_specs=placed,
            out_specs=P(sp, "tp"),
            check_vma=False,
        )(*arrays)

    return whole
```

```python
import functools

import jax
import jax.numpy as jnp
from jax import lax
from jax.experimental import pallas as pl
from jax.experimental.pallas import tpu as pltpu
from jax.sharding import Mesh
from jax.sharding import PartitionSpec as P

HEAD_DIM = 128
SPAN = 128
EPSILON = 1e-06
NT = (((1,), (1,)), ((), ()))
TN = (((0,), (0,)), ((), ()))
NN = (((1,), (0,)), ((), ()))


def dot(a, b, dims=NN):
    return lax.dot_general(a, b, dims, preferred_element_type=jnp.float32)


def lower_triangle():
    rows = lax.broadcasted_iota(jnp.int32, (SPAN, SPAN), 0)
    columns = lax.broadcasted_iota(jnp.int32, (SPAN, SPAN), 1)
    return rows >= columns


def decays(logits, gap, surge, causal):
    keys = gap / (1.0 + jnp.exp(logits.astype(jnp.float32)))
    series = keys * (1.0 / 7.0) + (1.0 / 6.0)
    for order in (5, 4, 3, 2):
        series = series * keys + (1.0 / order)
    logs = -(series * keys + 1.0) * keys
    high = logs.astype(jnp.bfloat16)
    low = (logs - high.astype(jnp.float32)).astype(jnp.bfloat16)
    ones = causal.astype(jnp.bfloat16)
    surged = jnp.sum(jnp.where(causal, surge, 0.0), axis=1, keepdims=True)
    return keys, dot(ones, high) + dot(ones, low) + surged


def head_state(lanes, head, rows, forget_ref, value_ref, gap_ref, surge_ref):
    causal = lower_triangle()
    gap = gap_ref[head]
    state = jnp.zeros((HEAD_DIM, HEAD_DIM), jnp.float32)
    total = jnp.zeros((1, HEAD_DIM), jnp.float32)
    for start in range(0, rows, SPAN):
        span = pl.ds(start, SPAN)
        keys, running = decays(forget_ref[span, lanes], gap, surge_ref[head, :, span], causal)
        ending = running[SPAN - 1 : SPAN, :]
        kept = (keys * jnp.exp(ending - running)).astype(jnp.bfloat16)
        state = state * jnp.exp(ending) + dot(value_ref[span, lanes], kept, TN)
        total = total + ending
    return state, total


def head_output(
    lanes, head, rows, query_ref, forget_ref, value_ref, gate_ref, gap_ref, surge_ref, gain, state, put
):
    causal = lower_triangle()
    gap = gap_ref[head]
    middle = SPAN // 2
    for start in range(0, rows, SPAN):
        span = pl.ds(start, SPAN)
        keys, running = decays(forget_ref[span, lanes], gap, surge_ref[head, :, span], causal)
        anchor = running[middle - 1 : middle, :]
        ending = running[SPAN - 1 : SPAN, :]
        logits = query_ref[span, lanes].astype(jnp.float32)
        queries = logits * (HEAD_DIM**-0.5) / (1.0 + jnp.exp(-logits))
        reach = queries * jnp.exp(running - anchor)
        back = keys * jnp.exp(anchor - running)
        values = value_ref[span, lanes]
        scores = dot(reach.astype(jnp.bfloat16), back.astype(jnp.bfloat16), NT)
        scores = jnp.where(causal, scores, 0.0).astype(jnp.bfloat16)
        inter = dot(
            (reach * jnp.exp(anchor)).astype(jnp.bfloat16), state.astype(jnp.bfloat16), NT
        )
        out = inter + dot(scores, values)
        if start + SPAN < rows:
            kept = (back * jnp.exp(ending - anchor)).astype(jnp.bfloat16)
            state = state * jnp.exp(ending) + dot(values, kept, TN)
        mean_sq = jnp.mean(out * out, axis=1, keepdims=True)
        gates = gate_ref[span, lanes].astype(jnp.float32)
        gates = gates / (1.0 + jnp.exp(-gates))
        put(span, (out * lax.rsqrt(mean_sq + EPSILON) * gain * gates).astype(jnp.bfloat16))


MESH_ID = pl.DeviceIdType.MESH


def front_kernel(
    sizes,
    query_in,
    forget_in,
    value_in,
    gate_in,
    gap_ref,
    surge_ref,
    gain_ref,
    weight_ref,
    projected_ref,
    parts_ref,
    whole_weight,
    state_out,
    total_out,
    state_in,
    total_in,
    carried,
    span_total,
    away,
    query_ref,
    forget_ref,
    value_ref,
    gate_ref,
    partial_out,
    partial_in,
    here,
    state_sems,
    total_sems,
    swap_sems,
    tp_sems,
    load_sems,
    weight_sems,
    partial_sems,
):
    hi_size, inner_size, tp_size, block = sizes
    sp_size = 2 * hi_size * inner_size
    rows, width = query_in.shape
    heads = width // HEAD_DIM
    half = heads // 2
    per = block // HEAD_DIM
    lo, inner, tp = (lax.axis_index(a) for a in ("lo", "inner", "tp"))
    place = (lax.axis_index("hi") * 2 + lo) * inner_size + inner

    def at(position):
        return {
            "hi": position // (2 * inner_size),
            "lo": (position // inner_size) % 2,
            "inner": position % inner_size,
        }

    shifts = [1]
    passed_back, passed_on = 0, 0
    by = 1
    while by < sp_size - 1:
        shifts.append(by)
        by *= 2
    strides = []
    stride = tp_size // 2
    while stride >= 1:
        strides.append(stride)
        stride //= 2

    def flipped(stride):
        return tp + stride - 2 * stride * ((tp // stride) % 2)

    line = hi_size * inner_size
    spot = lax.axis_index("hi") * inner_size + inner
    depth = weight_ref.shape[0]
    pieces, _, tile = partial_out.shape

    def slot(number):
        return pl.ds(pl.multiple_of(number * depth, depth), depth)

    loads = [
        pltpu.make_async_copy(source, target, load_sems.at[number])
        for number, (source, target) in enumerate(
            (
                (weight_ref, whole_weight.at[slot(spot)]),
                (forget_in, forget_ref),
                (value_in, value_ref),
                (query_in, query_ref),
                (gate_in, gate_ref),
            )
        )
    ]
    for load in loads:
        load.start()

    def on_line(position):
        return {"hi": position // inner_size, "inner": position % inner_size}

    def weight_copy(way, hop, piece):
        step = 1 if way == 0 else -1
        block = whole_weight.at[slot(spot - step * (hop - 1)), pl.ds(pl.multiple_of(piece * tile, tile), tile)]
        return pltpu.make_async_remote_copy(
            src_ref=block,
            dst_ref=block,
            send_sem=weight_sems.at[0, way, hop - 1, piece],
            recv_sem=weight_sems.at[1, way, hop - 1, piece],
            device_id=on_line(spot + step),
            device_id_type=MESH_ID,
        )

    def sends(way, hop):
        step = 1 if way == 0 else -1
        origin = spot - step * (hop - 1)
        target = spot + step
        return (origin >= 0) & (origin < line) & (target >= 0) & (target < line)

    def receives(way, hop):
        origin = spot - (1 if way == 0 else -1) * hop
        return (origin >= 0) & (origin < line)

    def send_weight(way, hop, piece):
        @pl.when(sends(way, hop))
        def _():
            weight_copy(way, hop, piece).start()

    def take_weight(hop, piece, ways=(0, 1)):
        for way in ways:

            @pl.when(receives(way, hop))
            def _():
                weight_copy(way, hop, piece).wait_recv()

            if hop + 1 < line:
                send_weight(way, hop + 1, piece)

    def take_hop(hop):
        for piece in range(pieces):
            take_weight(hop, piece)

    barrier = pltpu.get_barrier_semaphore()
    reaches = sorted(set(shifts + [inner_size]))
    neighbours = [spot + 1, spot - 1]
    peers = len(strides)
    for by in reaches:
        for there in (place + by, place - by):
            inside = (there >= 0) & (there < sp_size)

            @pl.when(inside)
            def _():
                pl.semaphore_signal(barrier, inc=1, device_id=at(there), device_id_type=MESH_ID)

            peers = peers + jnp.where(inside, 1, 0)
    for there in neighbours:
        inside = (there >= 0) & (there < line)

        @pl.when(inside)
        def _():
            pl.semaphore_signal(barrier, inc=1, device_id=on_line(there), device_id_type=MESH_ID)

        peers = peers + jnp.where(inside, 1, 0)
    for stride in strides:
        pl.semaphore_signal(
            barrier, inc=1, device_id={"tp": flipped(stride)}, device_id_type=MESH_ID
        )
    pl.semaphore_wait(barrier, peers)
    loads[0].wait()
    late = pieces // 2
    for piece in range(pieces):
        send_weight(1, 1, piece)
        if piece < late:
            send_weight(0, 1, piece)
    loads[1].wait()
    loads[2].wait()

    def lanes_of(head):
        return pl.ds(pl.multiple_of(head * HEAD_DIM, HEAD_DIM), HEAD_DIM)

    def state_body(head, carry):
        state, total = head_state(
            lanes_of(head), head, rows, forget_ref, value_ref, gap_ref, surge_ref
        )
        state_out[0, head] = state.astype(jnp.bfloat16)
        total_out[0, head] = jnp.broadcast_to(total, (8, HEAD_DIM))
        return carry

    lax.fori_loop(0, heads, state_body, 0)

    for turn, by in enumerate(shifts):
        copies = [
            pltpu.make_async_remote_copy(
                src_ref=source.at[turn],
                dst_ref=target.at[turn],
                send_sem=sems.at[0, turn],
                recv_sem=sems.at[1, turn],
                device_id=at(place + by),
                device_id_type=MESH_ID,
            )
            for source, target, sems in (
                (state_out, state_in, state_sems),
                (total_out, total_in, total_sems),
            )
        ]

        @pl.when(place + by < sp_size)
        def _():
            for copy in copies:
                copy.start()

        if late < pieces:
            send_weight(0, 1, late)
            late += 1
        elif line > 1:
            for _ in range(2 if turn + 1 == len(shifts) else 1):
                if passed_on < pieces:
                    take_weight(1, passed_on, (0,))
                    passed_on += 1
        if turn == 0:

            @pl.when(place == 0)
            def _():
                carried[...] = jnp.zeros_like(carried)
                span_total[...] = jnp.zeros_like(span_total)

        @pl.when(place - by >= 0)
        def _():
            for copy in copies:
                copy.wait_recv()

            def merge(head, carry):
                arrived = state_in[turn, head].astype(jnp.float32)
                passed = total_in[turn, head]
                if turn == 0:
                    carried[head] = arrived
                    span_total[head] = passed
                else:
                    carried[head] = arrived * jnp.exp(span_total[head, 0:1, :]) + carried[head]
                    span_total[head] = span_total[head] + passed
                return carry

            lax.fori_loop(0, heads, merge, 0)

        if turn + 1 < len(shifts):
            state_out[turn + 1] = carried[...].astype(jnp.bfloat16)
            total_out[turn + 1] = span_total[...]
            if line > 1 and turn >= 1 and turn - 1 < pieces:
                take_weight(1, turn - 1, (1,))
                passed_back = turn

    for piece in range(late, pieces):
        send_weight(0, 1, piece)
    if line > 1:
        for piece in range(pieces):
            if piece >= passed_back:
                take_weight(1, piece, (1,))
            if piece >= passed_on:
                take_weight(1, piece, (0,))
    loads[3].wait()
    loads[4].wait()
    gain = gain_ref[...]

    def compute(head, put):
        head_output(
            lanes_of(head),
            head,
            rows,
            query_ref,
            forget_ref,
            value_ref,
            gate_ref,
            gap_ref,
            surge_ref,
            gain,
            carried[head],
            put,
        )

    def head_of(chunk, parity):
        return (chunk // per * 2 + parity) * per + chunk % per

    def columns(chunk):
        return pl.ds(pl.multiple_of(chunk * HEAD_DIM, HEAD_DIM), HEAD_DIM)

    def swap_copy(chunk):
        return pltpu.make_async_remote_copy(
            src_ref=away.at[:, columns(chunk)],
            dst_ref=parts_ref.at[1, tp, :, columns(chunk)],
            send_sem=swap_sems.at[0, chunk],
            recv_sem=swap_sems.at[1, chunk],
            device_id={"lo": 1 - lo},
            device_id_type=MESH_ID,
        )

    def tp_copy(stage, which, mine, chunk):
        slot = tp
        for bit, stride in enumerate(strides[:stage]):
            if (mine >> bit) & 1:
                slot = slot + stride - 2 * stride * ((tp // stride) % 2)
        return pltpu.make_async_remote_copy(
            src_ref=parts_ref.at[which, slot, :, columns(chunk)],
            dst_ref=parts_ref.at[which, slot, :, columns(chunk)],
            send_sem=tp_sems.at[0, stage, which, mine, chunk],
            recv_sem=tp_sems.at[1, stage, which, mine, chunk],
            device_id={"tp": flipped(strides[stage])},
            device_id_type=MESH_ID,
        )

    def away_body(chunk, carry):
        def put(span, value):
            away[span, columns(chunk)] = value

        compute(head_of(chunk, 1 - lo), put)
        swap_copy(chunk).start()
        if line > 2 and pieces == half:
            take_weight(2, chunk, (1,))
        return carry

    lax.fori_loop(0, half, away_body, 0)

    def own_body(chunk, carry):
        def put(span, value):
            parts_ref[0, tp, span, columns(chunk)] = value

        compute(head_of(chunk, lo), put)
        for stage in range(len(strides)):
            tp_copy(stage, 0, 0, chunk).start()
        swap_copy(chunk).wait_recv()
        for stage in range(len(strides)):
            tp_copy(stage, 1, 0, chunk).start()
        return carry

    lax.fori_loop(0, half, own_body, 0)

    if line > 2:
        for piece in range(pieces):
            take_weight(2, piece, (0,) if pieces == half else (0, 1))

    for stage in range(len(strides)):

        def pass_body(chunk, carry):
            for which in (0, 1):
                for mine in range(1 << stage):
                    tp_copy(stage, which, mine, chunk).wait_recv()
                    for later in range(stage + 1, len(strides)):
                        tp_copy(later, which, mine | (1 << stage), chunk).start()
            return carry

        lax.fori_loop(0, half, pass_body, 0)

    for hop in range(3, line - 1):
        take_hop(hop)

    def partial_copy(piece):
        return pltpu.make_async_remote_copy(
            src_ref=partial_out.at[piece],
            dst_ref=partial_in.at[piece],
            send_sem=partial_sems.at[0, piece],
            recv_sem=partial_sems.at[1, piece],
            device_id={"lo": 1 - lo},
            device_id_type=MESH_ID,
        )

    def multiplied(which, piece):
        part_width = width // 2
        total = None
        for place in range(tp_size):
            block = whole_weight[pl.ds(place * part_width, part_width), pl.ds(piece * tile, tile)]
            term = dot(parts_ref[which, place], block)
            total = term if total is None else total + term
        return total

    for piece in range(pieces):
        if line > 3:
            take_weight(line - 1, piece)
        partial_out[piece] = multiplied(1, piece).astype(jnp.bfloat16)
        partial_copy(piece).start()
        here[piece] = multiplied(0, piece)
    for piece in range(pieces):
        partial_copy(piece).wait_recv()
        total = here[piece] + partial_in[piece].astype(jnp.float32)
        projected_ref[:, pl.ds(piece * tile, tile)] = total.astype(jnp.bfloat16)

    for piece in range(pieces):
        partial_copy(piece).wait_send()
        for way in (0, 1):
            for hop in range(1, line):

                @pl.when(sends(way, hop))
                def _():
                    weight_copy(way, hop, piece).wait_send()

    for turn, by in enumerate(shifts):

        @pl.when(place + by < sp_size)
        def _():
            for source, target, sems in (
                (state_out, state_in, state_sems),
                (total_out, total_in, total_sems),
            ):
                pltpu.make_async_remote_copy(
                    src_ref=source.at[turn],
                    dst_ref=target.at[turn],
                    send_sem=sems.at[0, turn],
                    recv_sem=sems.at[1, turn],
                    device_id=at(place + by),
                    device_id_type=MESH_ID,
                ).wait_send()

    def sent_body(chunk, carry):
        swap_copy(chunk).wait_send()
        for stage in range(len(strides)):
            for which in (0, 1):
                for mine in range(1 << stage):
                    tp_copy(stage, which, mine, chunk).wait_send()
        return carry

    lax.fori_loop(0, half, sent_body, 0)


def front(
    sizes, query_logits, forget_logits, value_inputs, gate_logits, gap, surge, gain, weight
):
    hi_size, inner_size, tp_size, block = sizes
    rows, width = query_logits.shape
    heads = width // HEAD_DIM
    turns = 1 + (2 * hi_size * inner_size - 2).bit_length()
    stages = tp_size.bit_length() - 1
    vmem = pl.BlockSpec(memory_space=pltpu.VMEM)
    anywhere = pl.BlockSpec(memory_space=pl.ANY)
    state = (heads, HEAD_DIM, HEAD_DIM)
    line = hi_size * inner_size
    depth, columns = weight.shape
    tile = 256
    pieces = columns // tile
    return pl.pallas_call(
        functools.partial(front_kernel, sizes),
        in_specs=[anywhere] * 4 + [vmem] * 3 + [anywhere],
        out_specs=vmem,
        out_shape=jax.ShapeDtypeStruct((rows, columns), jnp.bfloat16),
        scratch_shapes=[
            pltpu.VMEM((2, tp_size, rows, width // 2), jnp.bfloat16),
            pltpu.VMEM((line * depth, columns), jnp.bfloat16),
            pltpu.VMEM((turns,) + state, jnp.bfloat16),
            pltpu.VMEM((turns, heads, 8, HEAD_DIM), jnp.float32),
            pltpu.VMEM((turns,) + state, jnp.bfloat16),
            pltpu.VMEM((turns, heads, 8, HEAD_DIM), jnp.float32),
            pltpu.VMEM(state, jnp.float32),
            pltpu.VMEM((heads, 8, HEAD_DIM), jnp.float32),
            pltpu.VMEM((rows, width // 2), jnp.bfloat16),
            pltpu.VMEM((rows, width), jnp.bfloat16),
            pltpu.VMEM((rows, width), jnp.bfloat16),
            pltpu.VMEM((rows, width), jnp.bfloat16),
            pltpu.VMEM((rows, width), jnp.bfloat16),
            pltpu.VMEM((pieces, rows, tile), jnp.bfloat16),
            pltpu.VMEM((pieces, rows, tile), jnp.bfloat16),
            pltpu.VMEM((pieces, rows, tile), jnp.float32),
            pltpu.SemaphoreType.DMA((2, turns)),
            pltpu.SemaphoreType.DMA((2, turns)),
            pltpu.SemaphoreType.DMA((2, heads // 2)),
            pltpu.SemaphoreType.DMA((2, stages, 2, tp_size // 2, heads // 2)),
            pltpu.SemaphoreType.DMA((5,)),
            pltpu.SemaphoreType.DMA((2, 2, max(1, line - 1), pieces)),
            pltpu.SemaphoreType.DMA((2, pieces)),
        ],
        name="front",
        compiler_params=pltpu.CompilerParams(
            collective_id=0, has_side_effects=True, vmem_limit_bytes=64000 * 1024
        ),
        cost_estimate=pl.CostEstimate(
            flops=rows * width * 2000, bytes_accessed=8 * rows * width, transcendentals=0
        ),
    )(query_logits, forget_logits, value_inputs, gate_logits, gap, surge, gain, weight)


def per_device(
    hi_size,
    inner_size,
    tp_size,
    query_logits,
    forget_logits,
    value_inputs,
    output_gate_logits,
    forget_floor_gap,
    surge_log_decay,
    head_norm_gain,
    output_matrix,
    branch_norm_gain,
    residual,
):
    rows, width = query_logits.shape
    heads = width // HEAD_DIM
    column = lax.axis_index("tp")
    gap = lax.dynamic_slice_in_dim(
        forget_floor_gap.reshape(-1, 1, HEAD_DIM), column * heads, heads, axis=0
    )
    projected = front(
        (hi_size, inner_size, tp_size, inner_size * output_matrix.shape[0]),
        query_logits,
        forget_logits,
        value_inputs,
        output_gate_logits,
        gap,
        surge_log_decay.reshape(heads, 1, rows),
        head_norm_gain.reshape(1, HEAD_DIM),
        output_matrix,
    )
    branch = lax.optimization_barrier(projected).astype(jnp.float32)
    squares = lax.psum(jnp.sum(branch * branch, axis=1), "tp")
    columns = branch.shape[1]
    scale = lax.rsqrt(squares / (columns * tp_size) + EPSILON)
    gain_part = lax.dynamic_slice_in_dim(branch_norm_gain, column * columns, columns)
    return (residual.astype(jnp.float32) + branch * scale[:, None] * gain_part).astype(jnp.bfloat16)


def solution(mesh):
    sp_size, tp_size = mesh.shape["sp"], mesh.shape["tp"]
    sp = ("hi", "lo", "inner")
    placed = (
        P(sp, "tp"),
        P(sp, "tp"),
        P(sp, "tp"),
        P(sp, "tp"),
        P(),
        P("tp", sp),
        P(),
        P(sp, "tp"),
        P(),
        P(sp, "tp"),
    )

    def whole(*arrays):
        inner = max(1, HEAD_DIM * sp_size // arrays[7].shape[0])
        hi = sp_size // (2 * inner)
        devices = mesh.devices.reshape(hi, 2, inner, tp_size)
        paired = Mesh(devices, ("hi", "lo", "inner", "tp"))
        return jax.shard_map(
            functools.partial(per_device, hi, inner, tp_size),
            mesh=paired,
            in_specs=placed,
            out_specs=P(sp, "tp"),
            check_vma=False,
        )(*arrays)

    return whole
```
